32 devices in a mesh: dp: 4 (over y, x), kv: 4 (over z), tp: 2 (over core).
Axes of the slice: x: 2, y: 2, z: 4, core: 2. Of those that a mesh axis runs over, the one named last changes fastest.
Arguments:
- tokens: bfloat16 [32, 4, 2048], P('dp', None, 'kv'), may hold values from -420 to 420
- input_norm_gain: bfloat16 [2048], replicated, may hold values from 0.099609375 to 1.8984375
- head_input_weight: bfloat16 [2048, 3072], P('kv', 'tp'), may hold values from -0.125 to 0.125
- output_gate_weight: bfloat16 [2048, 3072], P('kv', 'tp'), may hold values from -0.125 to 0.125
- state_maps_weight: bfloat16 [2048, 2, 1024], P('kv', None, 'tp'), may hold values from -0.125 to 0.125
- step_size_weight: bfloat16 [2048, 48], replicated, may hold values from -0.125 to 0.125
- step_size_bias: float32 [48], replicated, may hold values from -4 to -1
- head_decay_speed: float32 [48], replicated, may hold values from 0.3 to 8
- proposal_decay_total: float32 [32, 4, 48], P(('dp', 'kv'), None, 'tp'), may hold values from -0.7 to 0
- head_input_kernel: bfloat16 [4, 3072], replicated, may hold values from -3 to 3
- state_maps_kernel: bfloat16 [4, 2, 1024], replicated, may hold values from -3 to 3
- head_direct_gain: float32 [48], replicated, may hold values from 0.5 to 1.5
- grouped_norm_gain: bfloat16 [3072], replicated, may hold values from 0.099609375 to 1.8984375
- output_weight: bfloat16 [3072, 2048], P('tp', 'kv'), may hold values from -0.109375 to 0.109375
- prior_state_value: float32 [32, 48, 64, 128], P(('dp', 'kv'), 'tp'), may hold values from -2.4 to 2.4
- previous_head_input: bfloat16 [32, 4, 3072], P(('dp', 'kv'), None, 'tp'), may hold values from -2.390625 to 2.390625
- previous_input_maps: bfloat16 [32, 4, 1024], P(('dp', 'kv'), None, 'tp'), may hold values from -5 to 5
- previous_log_decays: float32 [32, 4, 48], P(('dp', 'kv'), None, 'tp'), may hold values from -1.5 to -0.05
- prior_heads_window: bfloat16 [32, 7, 3072], P(('dp', 'kv'), None, 'tp'), may hold values from -6 to 6
- prior_maps_window: bfloat16 [32, 7, 2, 1024], P(('dp', 'kv'), None, None, 'tp'), may hold values from -6 to 6
- accepted: int32 [32], P(('dp', 'kv')), may hold values from 1 to 4
Outputs:
- mixed: bfloat16 [32, 4, 2048], P('dp', None, 'kv')
- accepted_state: float32 [32, 48, 64, 128], P(('dp', 'kv'), 'tp')
- current_head_input: bfloat16 [32, 4, 3072], P(('dp', 'kv'), None, 'tp')
- current_input_maps: bfloat16 [32, 4, 1024], P(('dp', 'kv'), None, 'tp')
- current_log_decays: float32 [32, 4, 48], P(('dp', 'kv'), None, 'tp')
- current_heads_window: bfloat16 [32, 7, 3072], P(('dp', 'kv'), None, 'tp')
- current_maps_window: bfloat16 [32, 7, 2, 1024], P(('dp', 'kv'), None, None, 'tp')
The draws below stay inside these ranges and needn't reach their ends.
All inputs are finite; a program needn't handle non-finite values.
Results may differ from the reference program's by a relative error of at most 0.029.
Values may be sent and summed in bfloat16 or wider, within the bound.
No kernel may reach another device: no remote copies, remote signals or barrier semaphores. Data moves between devices by JAX's collectives and lax.ppermute only.
A program may use at most 64 MiB of HBM per device.

```python
import math
import jax
import jax.numpy as jnp
from jax import lax

D = 2048
HEADS = 48
HEAD_DIM = 64
STATE = 128
CONV = 4
PROPOSALS = 4
BATCH = 32
INNER = 3072
BC_WIDTH = 1024
N_KV = 4
N_TP = 2


def draw_tokens(key, part):
    key_base, key_rows = jax.random.split(key, 2)
    columns = jnp.arange(D, dtype=jnp.float32) / D
    base = jnp.clip(jax.random.normal(key_base, (BATCH, PROPOSALS, D), jnp.float32), -4.0, 4.0)
    col_scale = 10.0 ** columns
    row_scale = jnp.exp(jax.random.uniform(key_rows, (BATCH, PROPOSALS, 1), jnp.float32, 0.0, math.log(10.0)))
    return (base * col_scale * row_scale).astype(jnp.bfloat16)


def draw_proposal_decay_total(key, part):
    key_pick, key_size = jax.random.split(key)
    pick = jax.random.randint(key_pick, (BATCH, PROPOSALS, HEADS), 0, 6)
    amounts = jnp.log(jax.random.uniform(key_size, (BATCH, PROPOSALS, HEADS), jnp.float32, 0.5, 0.8))
    return jnp.where(pick == 0, amounts, 0.0).astype(jnp.float32)


def touch_ends(result, own_key, low, largest):
    shape = result.shape
    spot = [jax.random.randint(jax.random.fold_in(own_key, axis), (), 0, shape[axis]) for axis in range(len(shape))]
    result = result.at[tuple(spot)].set(low)
    longest = shape.index(max(shape))
    spot[longest] = (spot[longest] + 1) % shape[longest]
    return result.at[tuple(spot)].set(largest)


def shard_levels(key, extent, shards, least, high):
    gain = 1.0
    for dim, blocks in shards:
        steps = jax.random.uniform(jax.random.fold_in(jax.random.fold_in(key, 6), dim), (blocks,), jnp.float32, least / len(shards), high / len(shards))
        gain = gain * jnp.repeat(jnp.exp(steps), extent[dim] // blocks).reshape((-1,) + (1,) * (len(extent) - 1 - dim))
    return gain


def noise(key, extent, deviation, limit, shards=(), kind=jnp.bfloat16):
    values = jax.random.normal(key, extent, jnp.float32) * deviation
    if len(shards) > 0:
        values = shard_levels(key, extent, shards, -0.22, 0.18) * values
    return jnp.clip(values, min=-limit, max=limit).astype(kind)


def setup_inputs(seed: int = 0) -> dict:
    arg_keys = jax.random.split(jax.random.key(seed), 22)
    tokens = draw_tokens(jax.random.fold_in(arg_keys[21], 71), 0)
    input_norm_gain = jnp.clip(1.0 + 0.18 * jax.random.normal(arg_keys[1], (D,), jnp.float32), 0.099609375, 1.8984375).astype(jnp.bfloat16)
    head_input_weight = noise(arg_keys[2], (D, INNER), D ** -0.5, 0.125, ((0, 4), (1, 2)))
    output_gate_weight = noise(arg_keys[3], (D, INNER), D ** -0.5, 0.125, ((0, 4), (1, 2)))
    state_maps_weight = noise(arg_keys[4], (D, 2, BC_WIDTH), D ** -0.5, 0.125, ((0, 4), (2, 2)))
    step_size_weight = noise(arg_keys[5], (D, HEADS), D ** -0.5, 0.125)
    step_size_bias = jnp.clip(jax.random.uniform(arg_keys[6], (HEADS,), jnp.float32, -4.0, -1.0), -4.0, -1.0)
    head_decay_speed = jnp.clip(jnp.exp(jax.random.uniform(arg_keys[7], (HEADS,), jnp.float32, math.log(0.3), math.log(8.0))), 0.3, 8.0)
    proposal_decay_total = draw_proposal_decay_total(jax.random.fold_in(arg_keys[21], 71), 0)
    head_input_kernel = noise(arg_keys[9], (CONV, INNER), CONV ** -0.5, 3.0)
    state_maps_kernel = noise(arg_keys[10], (CONV, 2, BC_WIDTH), CONV ** -0.5, 3.0)
    head_direct_gain = jnp.clip(jax.random.uniform(arg_keys[11], (HEADS,), jnp.float32, 0.5, 1.5), 0.5, 1.5)
    grouped_norm_gain = jnp.clip(1.0 + 0.18 * jax.random.normal(arg_keys[12], (INNER,), jnp.float32), 0.099609375, 1.8984375).astype(jnp.bfloat16)
    output_weight = noise(arg_keys[13], (INNER, D), INNER ** -0.5, 0.109375, ((0, 2), (1, 4)))
    prior_state_value = noise(arg_keys[14], (BATCH, HEADS, HEAD_DIM, STATE), 0.3, 2.4, ((0, 16), (1, 2)), jnp.float32)
    previous_head_input = noise(arg_keys[15], (BATCH, PROPOSALS, INNER), 0.3, 2.390625, ((0, 16), (2, 2)))
    previous_input_maps = noise(arg_keys[16], (BATCH, PROPOSALS, BC_WIDTH), 0.7, 5.0, ((0, 16), (2, 2)))
    previous_log_decays = jnp.clip(-1.5 + 1.45 * jax.random.uniform(arg_keys[17], (BATCH, PROPOSALS, HEADS), jnp.float32) ** shard_levels(arg_keys[17], (BATCH, PROPOSALS, HEADS), ((0, 16), (2, 2)), -0.2, 0.2), -1.5, -0.05)
    prior_heads_window = noise(arg_keys[18], (BATCH, CONV - 1 + PROPOSALS, INNER), 1.0, 6.0, ((0, 16), (2, 2)))
    prior_maps_window = noise(arg_keys[19], (BATCH, CONV - 1 + PROPOSALS, 2, BC_WIDTH), 1.0, 6.0, ((0, 16), (3, 2)))
    accepted = touch_ends(jax.random.randint(arg_keys[20], (BATCH,), 1, PROPOSALS + 1), jax.random.fold_in(arg_keys[20], 1), 1, PROPOSALS).astype(jnp.int32)
    return dict(tokens=tokens, input_norm_gain=input_norm_gain, head_input_weight=head_input_weight, output_gate_weight=output_gate_weight, state_maps_weight=state_maps_weight, step_size_weight=step_size_weight, step_size_bias=step_size_bias, head_decay_speed=head_decay_speed, proposal_decay_total=proposal_decay_total, head_input_kernel=head_input_kernel, state_maps_kernel=state_maps_kernel, head_direct_gain=head_direct_gain, grouped_norm_gain=grouped_norm_gain, output_weight=output_weight, prior_state_value=prior_state_value, previous_head_input=previous_head_input, previous_input_maps=previous_input_maps, previous_log_decays=previous_log_decays, prior_heads_window=prior_heads_window, prior_maps_window=prior_maps_window, accepted=accepted)


eps = 1e-06

def pick_tail(history, accepted):
    rows = history.shape[1]
    keep = CONV - 1
    index = jnp.arange(rows, dtype=jnp.int32)
    offsets = jnp.arange(keep, dtype=jnp.int32)
    select = (index[None, None, :] == accepted[:, None, None] + offsets[None, :, None]).astype(jnp.float32)
    flat = history.astype(jnp.float32).reshape(history.shape[0], rows, -1)
    picked = jnp.einsum('skr,src->skc', select, flat, precision=lax.Precision.HIGHEST)
    return picked.reshape((history.shape[0], keep) + history.shape[2:])

def causal_conv(window, weight):
    length = window.shape[1] - CONV + 1
    total = weight[0] * window[:, 0:length]
    for offset in range(1, CONV):
        total = total + weight[offset] * window[:, offset:offset + length]
    return jax.nn.silu(total)

def local_mixer_output(unfiltered_heads, gate_logits, unfiltered_maps, step_logits, prior_heads_window, prior_maps_window, accepted, proposal_run, prior_state_value, previous_head_input, previous_input_maps, previous_log_decays, head_input_kernel, state_maps_kernel, step_size_bias, head_decay_speed, head_direct_gain, grouped_norm_gain):
    seqs, props, width = unfiltered_heads.shape
    heads = step_logits.shape[2]
    groups = unfiltered_maps.shape[3] // STATE
    repeat = heads // groups
    tail_x = pick_tail(prior_heads_window, accepted)
    tail_bc = pick_tail(prior_maps_window, accepted)
    window_x = jnp.concatenate([tail_x, unfiltered_heads.astype(jnp.float32)], axis=1)
    window_bc = jnp.concatenate([tail_bc, unfiltered_maps.astype(jnp.float32)], axis=1)
    current_heads_window = window_x.astype(jnp.bfloat16)
    current_maps_window = window_bc.astype(jnp.bfloat16)
    x_conv = causal_conv(window_x, head_input_kernel.astype(jnp.float32)).reshape(seqs, props, heads, HEAD_DIM)
    bc_conv = causal_conv(window_bc, state_maps_kernel.astype(jnp.float32)).reshape(seqs, props, 2, groups, STATE)
    b_conv = bc_conv[:, :, 0]
    c_conv = bc_conv[:, :, 1]
    positive_step_size = jax.nn.softplus(step_logits + step_size_bias)
    logarithm_decay = proposal_run - head_decay_speed * positive_step_size
    weighted = positive_step_size[..., None] * x_conv
    current_head_input = weighted.reshape(seqs, props, width).astype(jnp.bfloat16)
    current_input_maps = b_conv.reshape(seqs, props, groups * STATE).astype(jnp.bfloat16)
    past_heads = previous_head_input.astype(jnp.float32).reshape(seqs, props, heads, HEAD_DIM)
    past_keys = jnp.repeat(previous_input_maps.astype(jnp.float32).reshape(seqs, props, groups, STATE), repeat, axis=2)
    carried = prior_state_value
    for position in range(props):
        keep = (position < accepted).astype(jnp.float32)[:, None]
        factor = jnp.exp(keep * previous_log_decays[:, position])
        update = past_heads[:, position, :, :, None] * past_keys[:, position, :, None, :]
        carried = carried * factor[:, :, None, None] + keep[:, :, None, None] * update
    cumulative = jnp.cumsum(logarithm_decay, axis=1)
    c_heads = jnp.repeat(c_conv, repeat, axis=2)
    b_heads = jnp.repeat(b_conv, repeat, axis=2)
    from_state = jnp.exp(cumulative)[..., None] * jnp.einsum('sthn,shpn->sthp', c_heads, carried, precision=lax.Precision.HIGHEST)
    order = jnp.arange(props)
    causal = (order[:, None] >= order[None, :])[None, :, :, None]
    spread_log = cumulative[:, :, None, :] - cumulative[:, None, :, :]
    decay = jnp.where(causal, jnp.exp(jnp.where(causal, spread_log, 0.0)), 0.0)
    scores = jnp.einsum('sthn,suhn->stuh', c_heads, b_heads, precision=lax.Precision.HIGHEST) * decay
    within = jnp.einsum('stuh,suhp->sthp', scores, weighted, precision=lax.Precision.HIGHEST)
    heads_out = from_state + within + head_direct_gain[:, None] * x_conv
    gated = heads_out.reshape(seqs, props, width) * jax.nn.silu(gate_logits)
    grouped = gated.reshape(seqs, props, groups, width // groups)
    grouped = grouped * lax.rsqrt(lax.optimization_barrier(jnp.mean(grouped * grouped, axis=-1, keepdims=True)) + eps)
    normalized_input = (grouped.reshape(seqs, props, width) * grouped_norm_gain.astype(jnp.float32)).astype(jnp.bfloat16)
    return (normalized_input, carried, current_head_input, current_input_maps, logarithm_decay, current_heads_window, current_maps_window)

def reference(tokens, input_norm_gain, head_input_weight, output_gate_weight, state_maps_weight, step_size_weight, step_size_bias, head_decay_speed, proposal_decay_total, head_input_kernel, state_maps_kernel, head_direct_gain, grouped_norm_gain, output_weight, prior_state_value, previous_head_input, previous_input_maps, previous_log_decays, prior_heads_window, prior_maps_window, accepted):
    values = tokens.astype(jnp.float32)
    inv_rms = lax.rsqrt(lax.optimization_barrier(jnp.sum(values * values, axis=-1)) / D + eps).reshape(BATCH * PROPOSALS, 1)
    scaled = (values * input_norm_gain.astype(jnp.float32)).astype(jnp.bfloat16).reshape(BATCH * PROPOSALS, D)
    w_all = jnp.concatenate([head_input_weight, output_gate_weight, state_maps_weight.reshape(D, 2 * BC_WIDTH), step_size_weight], axis=1)
    feat_block = D // N_KV
    proj = jnp.zeros((BATCH * PROPOSALS, w_all.shape[1]), jnp.float32)
    for kv_part in range(N_KV):
        partial_value = jnp.dot(scaled[:, kv_part * feat_block:(kv_part + 1) * feat_block], w_all[kv_part * feat_block:(kv_part + 1) * feat_block], preferred_element_type=jnp.float32)
        proj = proj + partial_value.astype(jnp.bfloat16).astype(jnp.float32)
    proj_x = proj[:, 0:INNER]
    proj_gate = proj[:, INNER:2 * INNER]
    proj_bc = proj[:, 2 * INNER:2 * INNER + 2 * BC_WIDTH]
    proj_step = proj[:, 2 * INNER + 2 * BC_WIDTH:]
    unfiltered_heads = (proj_x * inv_rms).astype(jnp.bfloat16).reshape(BATCH, PROPOSALS, INNER)
    gate_logits = (proj_gate * inv_rms).reshape(BATCH, PROPOSALS, INNER)
    unfiltered_maps = (proj_bc * inv_rms).astype(jnp.bfloat16).reshape(BATCH, PROPOSALS, 2, BC_WIDTH)
    step_logits = (proj_step * inv_rms).reshape(BATCH, PROPOSALS, HEADS)

    def single_sequence(items):
        outs = local_mixer_output(*(item[None] for item in items), head_input_kernel, state_maps_kernel, step_size_bias, head_decay_speed, head_direct_gain, grouped_norm_gain)
        return tuple((out[0] for out in outs))
    normalized_input, accepted_state, current_head_input, current_input_maps, current_log_decays, current_heads_window, current_maps_window = lax.map(single_sequence, (unfiltered_heads, gate_logits, unfiltered_maps, step_logits, prior_heads_window, prior_maps_window, accepted, proposal_decay_total, prior_state_value, previous_head_input, previous_input_maps, previous_log_decays))
    block = INNER // N_TP
    flat = normalized_input.reshape(BATCH * PROPOSALS, INNER)
    total = jnp.zeros((BATCH * PROPOSALS, D), jnp.float32)
    for part_index in range(N_TP):
        partial_value = jnp.dot(flat[:, part_index * block:(part_index + 1) * block], output_weight[part_index * block:(part_index + 1) * block], preferred_element_type=jnp.float32)
        total = total + partial_value.astype(jnp.bfloat16).astype(jnp.float32)
    mixed = total.astype(jnp.bfloat16).reshape(BATCH, PROPOSALS, D)
    return (mixed, accepted_state, current_head_input, current_input_maps, current_log_decays, current_heads_window, current_maps_window)
```

```python
import functools

import jax
import jax.numpy as jnp
from jax import lax
from jax.experimental import pallas as pl
from jax.experimental.pallas import tpu as pltpu
from jax.sharding import PartitionSpec as P

HEAD_DIM = 64
STATE = 128
CONV = 4
LANES = 128
DIRECT = 8

eps = 1e-06
f32 = jnp.float32
bf16 = jnp.bfloat16

NT = (((1,), (1,)), ((), ()))
TN = (((0,), (0,)), ((), ()))


def params(mib):
    return pltpu.CompilerParams(vmem_limit_bytes=mib << 20)


def peer(me, k, n, back=False):
    if n > DIRECT:
        return k
    if n & (n - 1) == 0:
        return me ^ k
    return lax.rem(me + (n - k if back else k), n)


def permute(array, axis, k, n):
    return lax.ppermute(array, axis, [(i, int(peer(i, k, n))) for i in range(n)])


def pick(rows, index, count, width):
    out = rows[:, :width]
    for block in range(1, count):
        out = jnp.where(index == block, rows[:, block * width : (block + 1) * width], out)
    return out


def spread(values, heads):
    rows = values.shape[0]
    per = LANES // HEAD_DIM
    lane = lax.broadcasted_iota(jnp.int32, (rows, LANES), 1)
    tiles = []
    for first in range(0, heads, per):
        tile = jnp.broadcast_to(values[:, first : first + 1], (rows, LANES))
        for j in range(1, per):
            other = jnp.broadcast_to(values[:, first + j : first + j + 1], (rows, LANES))
            tile = jnp.where(lane >= j * HEAD_DIM, other, tile)
        tiles.append(tile)
    return jnp.concatenate(tiles, axis=1)


def silu(x):
    return x * (1.0 / (1.0 + jnp.exp(-x)))


def project_kernel(n_kv, n_heads, tok, gain, wx, wm, wg, ws, *outs):
    kv = lax.axis_index("kv")
    seqs, props, local_d = tok.shape
    own = seqs // n_kv
    rows = own * props
    parts, squares = [], []
    for k in range(n_kv):
        start = peer(kv, k, n_kv) * own
        for s in range(own):
            values = tok[start + s].astype(f32)
            parts.append(values)
    values = jnp.concatenate(parts, axis=0)
    squares = jnp.sum(values * values, axis=1, keepdims=True)
    scaled = (values * gain[...]).astype(bf16)
    high = squares.astype(bf16).astype(f32)
    step = lax.dot_general(scaled, ws[...], NT, preferred_element_type=f32)
    lane = lax.broadcasted_iota(jnp.int32, step.shape, 1)
    step = jnp.where(lane == n_heads, high, jnp.where(lane == n_heads + 1, squares - high, step))
    at = 0
    for block in (wx, wm, wg):
        width = block.shape[1]
        part = jnp.dot(scaled, block[...], preferred_element_type=f32)
        for k in range(n_kv):
            outs[k][:, at : at + width] = part[k * rows : (k + 1) * rows].astype(bf16)
        at += width
    for k in range(n_kv):
        outs[k][:, at:] = step[k * rows : (k + 1) * rows].astype(bf16)


def state_kernel(
    n_tp,
    acc,
    state,
    past_x,
    past_maps,
    past_logs,
    heads_window,
    maps_window,
    head_taps,
    map_taps,
    bias,
    speed,
    direct,
    norm_gain,
    new_state,
    state_low,
    tail_x,
    tail_maps,
    conv_tail,
    taps,
    vectors,
    small,
    gain_rows,
):
    tp = lax.axis_index("tp")
    own, heads = state.shape[:2]
    props, width = past_x.shape[1:]
    bc = past_maps.shape[2]
    groups = bc // STATE
    per_group = heads // groups
    group_width = per_group * HEAD_DIM
    keep = CONV - 1

    head_cols = pl.ds(pl.multiple_of(tp * width, LANES), width)
    map_cols = pl.ds(pl.multiple_of(tp * bc, LANES), bc)
    weight_x = head_taps[:, head_cols].astype(f32)
    taps[:, :width] = weight_x
    weight_b, weight_c = [], []
    for k in range(CONV):
        pair = map_taps[k, :, map_cols].astype(f32)
        weight_b.append(pair[0:1])
        weight_c.append(pair[1:2])
        taps[k : k + 1, width : width + bc] = pair[0:1]
        taps[k : k + 1, width + bc :] = pair[1:2]
    direct_half = pick(direct[...], tp, n_tp, heads)
    vectors[0:1, :] = spread(direct_half, heads)
    gain_rows[...] = norm_gain[...].astype(f32)
    per_row = width // LANES
    for j in range(per_row):
        vectors[1:2, j * LANES : (j + 1) * LANES] = gain_rows[pl.ds(tp * per_row + j, 1), :]
    small[0:1, :heads] = pick(bias[...], tp, n_tp, heads)
    small[1:2, :heads] = pick(speed[...], tp, n_tp, heads)

    for s in range(own):
        a = acc[s]
        xs, bs, cs = [], [], []
        for k in range(keep):
            row = heads_window[a + k].astype(f32)
            xs.append(row[s : s + 1])
            pair = maps_window[s, a + k]
            tail_maps[s, k] = pair
            pair = pair.astype(f32)
            bs.append(pair[0:1])
            cs.append(pair[1:2])
        for k in range(keep):
            tail_x[k, s : s + 1, :] = xs[k].astype(bf16)
        for at, weights, rows in (
            (0, [weight_x[k : k + 1] for k in range(CONV)], xs),
            (width, weight_b, bs),
            (width + bc, weight_c, cs),
        ):
            size = rows[0].shape[1]
            for t in range(props):
                total = jnp.zeros((1, size), f32)
                for k in range(CONV):
                    if t + k < keep:
                        total = total + weights[k] * rows[t + k]
                conv_tail[s * props + t : s * props + t + 1, at : at + size] = total

        logs = past_logs[s]
        after = jnp.zeros((1, heads), f32)
        coefficients = [None] * props
        for j in reversed(range(props)):
            coefficients[j] = jnp.where(j < a, jnp.exp(after), 0.0)
            after = after + jnp.where(j < a, logs[j : j + 1], 0.0)
        factor = jnp.exp(after)
        coefficient = spread(jnp.concatenate(coefficients, axis=0), heads)
        scaled = past_x[s].astype(f32) * coefficient
        high = scaled.astype(bf16).astype(f32)
        left = jnp.concatenate([high, scaled - high], axis=0)
        maps = past_maps[s].astype(f32)
        maps = jnp.concatenate([maps, maps], axis=0).astype(bf16)
        for g in range(groups):
            block = left[:, g * group_width : (g + 1) * group_width]
            update = lax.dot_general(
                block.astype(bf16),
                maps[:, g * STATE : (g + 1) * STATE],
                TN,
                preferred_element_type=f32,
            )
            for i in range(per_group):
                h = g * per_group + i
                value = state[s, h] * factor[:, h : h + 1]
                value = value + update[i * HEAD_DIM : (i + 1) * HEAD_DIM]
                new_state[s, h] = value
                state_low[s, h * HEAD_DIM : (h + 1) * HEAD_DIM, :] = value.astype(bf16)


def mixer_kernel(
    n_features,
    n_blocks,
    decay_total,
    state_low,
    conv_tail,
    taps,
    vectors,
    small,
    *rest,
):
    blocks = rest[:n_blocks]
    normed, raw_out, weighted_out, maps_out, logs_out = rest[n_blocks:]
    own, _, heads = decay_total.shape
    rows, width = weighted_out.shape
    props = rows // own
    bc = (conv_tail.shape[1] - width) // 2
    groups = bc // STATE
    group_width = width // groups
    total = None
    for block in blocks:
        for piece in [block[...]] if len(block.shape) == 2 else [block[i] for i in range(block.shape[0])]:
            piece = piece.astype(f32)
            total = piece if total is None else total + piece
    conv_width = width + 2 * bc
    tail = total[:, conv_width + width :]
    squares = tail[:, heads : heads + 1] + tail[:, heads + 1 : heads + 2]
    inv_rms = lax.rsqrt(squares / n_features + eps)
    raw = (total[:, :conv_width] * inv_rms).astype(bf16)
    raw_out[...] = raw
    raw = raw.astype(f32)
    gate = total[:, conv_width : conv_width + width] * inv_rms

    step_pre = tail[:, :heads] * inv_rms + small[0:1, :heads]
    step = jnp.maximum(step_pre, 0.0) + jnp.log1p(jnp.exp(-jnp.abs(step_pre)))
    totals = jnp.concatenate([decay_total[s] for s in range(own)], axis=0)
    logs = totals - small[1:2, :heads] * step
    logs_out[...] = logs
    step = spread(step, heads)
    decay = spread(jnp.exp(logs), heads)

    def turn(value, d):
        return pltpu.roll(value, d, 0)

    def since(size):
        return lax.rem(lax.broadcasted_iota(jnp.int32, (rows, size), 0), props)

    pos = since(conv_width)
    conv = conv_tail[...] + taps[CONV - 1 : CONV] * raw
    for d in range(1, CONV):
        conv = conv + jnp.where(pos >= d, taps[CONV - 1 - d : CONV - d] * turn(raw, d), 0.0)
    conv = silu(conv)
    x_conv = conv[:, :width]
    b_conv = conv[:, width : width + bc]
    c_conv = conv[:, width + bc :]
    maps_out[...] = b_conv
    weighted = step * x_conv
    weighted_out[...] = weighted

    pos = since(width)
    c_low = c_conv.astype(bf16)
    row_seq = lax.broadcasted_iota(jnp.int32, (rows, group_width), 0) // props
    from_state = []
    for g in range(groups):
        left = c_low[:, g * STATE : (g + 1) * STATE]
        out = None
        for s in range(own):
            part = lax.dot_general(
                left,
                state_low[s, g * group_width : (g + 1) * group_width, :],
                NT,
                preferred_element_type=f32,
            )
            out = part if out is None else jnp.where(row_seq >= s, part, out)
        from_state.append(out)
    from_state = jnp.concatenate(from_state, axis=1)

    span = decay
    to_start = decay
    heads_out = vectors[0:1] * x_conv
    for d in range(props):
        product = c_conv * (b_conv if d == 0 else turn(b_conv, d))
        scores = jnp.concatenate(
            [
                jnp.broadcast_to(
                    jnp.sum(product[:, g * STATE : (g + 1) * STATE], axis=1, keepdims=True),
                    (rows, group_width),
                )
                for g in range(groups)
            ],
            axis=1,
        )
        if d == 0:
            heads_out = heads_out + scores * weighted
        else:
            term = scores * span * turn(weighted, d)
            heads_out = heads_out + jnp.where(pos >= d, term, 0.0)
            span = span * turn(decay, d)
            to_start = jnp.where(pos >= d, span, to_start)
    heads_out = heads_out + to_start * from_state
    gated = heads_out * silu(gate)
    for g in range(groups):
        lanes = slice(g * group_width, (g + 1) * group_width)
        part = gated[:, lanes]
        mean = jnp.sum(part * part, axis=1, keepdims=True) / group_width
        normed[:, lanes] = (part * lax.rsqrt(mean + eps) * vectors[1:2, lanes]).astype(bf16)


def outputs_kernel(
    raw, weighted, maps, logs, tail_x, tail_maps, head_input, input_maps, log_decays, heads_window, maps_window
):
    own, props, width = head_input.shape
    bc = input_maps.shape[2]
    keep = CONV - 1
    heads_window[:keep] = tail_x[...]
    rows = raw[...].astype(f32)
    weighted, maps, logs = weighted[...], maps[...], logs[...]
    for s in range(own):
        mine = slice(s * props, (s + 1) * props)
        head_input[s] = weighted[mine].astype(bf16)
        input_maps[s] = maps[mine].astype(bf16)
        log_decays[s] = logs[mine]
        maps_window[s, :keep] = tail_maps[s]
        for t in range(props):
            r = s * props + t
            pair = [rows[r : r + 1, width : width + bc], rows[r : r + 1, width + bc :]]
            maps_window[s, keep + t] = jnp.concatenate(pair, axis=0).astype(bf16)
    for t in range(props):
        both = [rows[s * props + t : s * props + t + 1, :width] for s in range(own)]
        heads_window[keep + t] = jnp.concatenate(both, axis=0).astype(bf16)


def mix_kernel(n_kv, weight, *rest):
    blocks, out = rest[:-1], rest[-1]
    kv = lax.axis_index("kv")
    _, props, _ = out.shape
    pieces = []
    for block in blocks:
        pieces += [block[...]] if len(block.shape) == 2 else [block[i] for i in range(block.shape[0])]
    rows = pieces[0].shape[0]
    own = rows // props
    left = jnp.concatenate([piece.astype(f32) for piece in pieces], axis=0).astype(bf16)
    part = jnp.dot(left, weight[...], preferred_element_type=f32)
    for k in range(n_kv):
        start = peer(kv, k, n_kv, back=True) * own
        for s in range(own):
            at = k * rows + s * props
            out[start + s] = part[at : at + props].astype(bf16)


def local(
    tokens,
    input_norm_gain,
    head_input_weight,
    output_gate_weight,
    state_maps_weight,
    step_size_weight,
    step_size_bias,
    head_decay_speed,
    proposal_decay_total,
    head_input_kernel,
    state_maps_kernel,
    head_direct_gain,
    grouped_norm_gain,
    output_weight,
    prior_state_value,
    previous_head_input,
    previous_input_maps,
    previous_log_decays,
    prior_heads_window,
    prior_maps_window,
    accepted,
):
    n_kv, n_tp = lax.axis_size("kv"), lax.axis_size("tp")
    kv, tp = lax.axis_index("kv"), lax.axis_index("tp")
    seqs, props, local_d = tokens.shape
    heads = step_size_weight.shape[1] // n_tp
    width = head_input_weight.shape[1]
    bc = state_maps_weight.shape[2]
    own = prior_state_value.shape[0]
    rows = own * props
    conv_width = width + 2 * bc
    packed = conv_width + width + LANES
    sds = jax.ShapeDtypeStruct
    vmem = pl.BlockSpec(memory_space=pltpu.VMEM)

    gain = lax.dynamic_slice_in_dim(input_norm_gain, kv * local_d, local_d, 0)
    gain = gain.astype(f32).reshape(1, local_d)
    step_part = lax.dynamic_slice(
        step_size_weight.T, (tp * heads, kv * local_d), (heads, local_d)
    )
    step_part = jnp.pad(step_part, ((0, LANES - heads), (0, 0)))
    sent = pl.pallas_call(
        functools.partial(project_kernel, n_kv, heads),
        out_shape=[sds((rows, packed), bf16)] * n_kv,
        compiler_params=params(8),
        name="project",
    )(
        tokens,
        gain,
        head_input_weight,
        state_maps_weight.reshape(local_d, 2 * bc),
        output_gate_weight,
        step_part,
    )
    if n_kv <= DIRECT:
        got = [permute(sent[k], "kv", k, n_kv) for k in reversed(range(1, n_kv))]
        got = [sent[0]] + got
    else:
        got = [lax.all_to_all(jnp.stack(sent), "kv", 0, 0)]

    (
        accepted_state,
        state_low,
        tail_x,
        tail_maps,
        conv_tail,
        taps,
        vectors,
        small,
    ) = pl.pallas_call(
        functools.partial(state_kernel, n_tp),
        out_shape=[
            sds(prior_state_value.shape, f32),
            sds((own, width, STATE), bf16),
            sds((CONV - 1, own, width), bf16),
            sds((own, CONV - 1, 2, bc), bf16),
            sds((rows, conv_width), f32),
            sds((CONV, conv_width), f32),
            sds((2, width), f32),
            sds((2, LANES), f32),
        ],
        in_specs=[pl.BlockSpec(memory_space=pltpu.SMEM)] + [vmem] * 12,
        scratch_shapes=[pltpu.VMEM((n_tp * width // LANES, LANES), f32)],
        compiler_params=params(12),
        name="state",
    )(
        accepted,
        prior_state_value,
        previous_head_input,
        previous_input_maps,
        previous_log_decays,
        jnp.transpose(prior_heads_window, (1, 0, 2)),
        prior_maps_window,
        head_input_kernel,
        state_maps_kernel,
        step_size_bias.reshape(1, -1),
        head_decay_speed.reshape(1, -1),
        head_direct_gain.reshape(1, -1),
        grouped_norm_gain.reshape(-1, LANES),
    )

    normed, raw, weighted, maps, logs = pl.pallas_call(
        functools.partial(mixer_kernel, local_d * n_kv, len(got)),
        out_shape=[
            sds((rows, width), bf16),
            sds((rows, conv_width), bf16),
            sds((rows, width), f32),
            sds((rows, bc), f32),
            sds((rows, heads), f32),
        ],
        compiler_params=params(8),
        name="mixer",
    )(proposal_decay_total, state_low, conv_tail, taps, vectors, small, *got)

    if n_kv <= DIRECT:
        gathered = [permute(normed, "kv", k, n_kv) for k in reversed(range(1, n_kv))]
        gathered = [normed] + gathered[::-1]
    else:
        gathered = [lax.all_gather(normed, "kv")]

    head_input, input_maps, log_decays, heads_window, maps_window = pl.pallas_call(
        outputs_kernel,
        out_shape=[
            sds((own, props, width), bf16),
            sds((own, props, bc), bf16),
            sds((own, props, heads), f32),
            sds((CONV - 1 + props, own, width), bf16),
            sds((own, CONV - 1 + props, 2, bc), bf16),
        ],
        compiler_params=params(8),
        name="outputs",
    )(raw, weighted, maps, logs, tail_x, tail_maps)

    part = pl.pallas_call(
        functools.partial(mix_kernel, n_kv),
        out_shape=sds((seqs, props, local_d), bf16),
        compiler_params=params(8),
        name="mix",
    )(output_weight, *gathered)
    total = part.astype(f32)
    for k in range(1, n_tp):
        total = total + permute(part, "tp", k, n_tp).astype(f32)
    return (
        total.astype(bf16),
        accepted_state,
        head_input,
        input_maps,
        log_decays,
        jnp.transpose(heads_window, (1, 0, 2)),
        maps_window,
    )


def solution(mesh):
    return jax.shard_map(
        local,
        mesh=mesh,
        in_specs=(
            P("dp", None, "kv"),
            P(),
            P("kv", "tp"),
            P("kv", "tp"),
            P("kv", None, "tp"),
            P(),
            P(),
            P(),
            P(("dp", "kv"), None, "tp"),
            P(),
            P(),
            P(),
            P(),
            P("tp", "kv"),
            P(("dp", "kv"), "tp", None, None),
            P(("dp", "kv"), None, "tp"),
            P(("dp", "kv"), None, "tp"),
            P(("dp", "kv"), None, "tp"),
            P(("dp", "kv"), None, "tp"),
            P(("dp", "kv"), None, None, "tp"),
            P(("dp", "kv")),
        ),
        out_specs=(
            P("dp", None, "kv"),
            P(("dp", "kv"), "tp", None, None),
            P(("dp", "kv"), None, "tp"),
            P(("dp", "kv"), None, "tp"),
            P(("dp", "kv"), None, "tp"),
            P(("dp", "kv"), None, "tp"),
            P(("dp", "kv"), None, None, "tp"),
        ),
        check_vma=False,
    )
```

```python
import functools

import jax
import jax.numpy as jnp
from jax import lax
from jax.experimental import pallas as pl
from jax.experimental.pallas import tpu as pltpu
from jax.sharding import PartitionSpec as P

HEAD_DIM = 64
STATE = 128
CONV = 4
LANES = 128
DIRECT = 8

eps = 1e-06
f32 = jnp.float32
bf16 = jnp.bfloat16

NT = (((1,), (1,)), ((), ()))
TN = (((0,), (0,)), ((), ()))


def params(mib):
    return pltpu.CompilerParams(vmem_limit_bytes=mib << 20)


def peer(me, k, n, back=False):
    if n > DIRECT:
        return k
    if n & (n - 1) == 0:
        return me ^ k
    return lax.rem(me + (n - k if back else k), n)


def permute(array, axis, k, n):
    return lax.ppermute(array, axis, [(i, int(peer(i, k, n))) for i in range(n)])


def pick(rows, index, count, width):
    out = rows[:, :width]
    for block in range(1, count):
        out = jnp.where(index == block, rows[:, block * width : (block + 1) * width], out)
    return out


def spread(values, heads):
    rows = values.shape[0]
    per = LANES // HEAD_DIM
    lane = lax.broadcasted_iota(jnp.int32, (rows, LANES), 1)
    tiles = []
    for first in range(0, heads, per):
        tile = jnp.broadcast_to(values[:, first : first + 1], (rows, LANES))
        for j in range(1, per):
            other = jnp.broadcast_to(values[:, first + j : first + j + 1], (rows, LANES))
            tile = jnp.where(lane >= j * HEAD_DIM, other, tile)
        tiles.append(tile)
    return jnp.concatenate(tiles, axis=1)


def silu(x):
    return x * (1.0 / (1.0 + jnp.exp(-x)))


def project_kernel(n_kv, n_tp, chunk, tok_hbm, gain_hbm, wx, wm, wg, ws_hbm, *rest):
    outs = rest[:n_kv]
    tok, gain, gain_rows, ws, step_rows, wide, pairs, sems = rest[n_kv:]
    kv, tp = lax.axis_index("kv"), lax.axis_index("tp")
    seqs, props, local_d = tok.shape
    own = seqs // n_kv
    rows = own * props
    width, bc = wx.shape[1], wm.shape[2]
    heads = ws.shape[0] // n_tp
    aligned = local_d % LANES == 0

    copies = []

    def fetch(source, target):
        copy = pltpu.make_async_copy(source, target, sems.at[len(copies)])
        copy.start()
        copies.append(copy)
        return copy

    small = [fetch(tok_hbm, tok), fetch(gain_hbm, gain)]
    columns = pl.ds(pl.multiple_of(kv * local_d, LANES), local_d) if aligned else slice(None)
    small.append(fetch(ws_hbm.at[:, columns], ws))
    maps = fetch(wm, pairs)
    plan = []
    for at in range(0, width, chunk):
        here = slice(at, at + chunk)
        plan.append((fetch(wx.at[:, here], wide.at[:, here]), at, here))
    for at in range(0, width, chunk):
        here = slice(width + at, width + at + chunk)
        plan.append((fetch(wg.at[:, at : at + chunk], wide.at[:, here]), width + 2 * bc + at, here))

    for copy in small:
        copy.wait()
    parts = []
    for k in range(n_kv):
        start = peer(kv, k, n_kv) * own
        for s in range(own):
            parts.append(tok[start + s].astype(f32))
    values = jnp.concatenate(parts, axis=0)
    squares = jnp.sum(values * values, axis=1, keepdims=True)
    gain_rows[...] = gain[...].astype(f32)
    if aligned:
        per = local_d // LANES
        factor = [gain_rows[pl.ds(kv * per + j, 1), :] for j in range(per)]
        factor = jnp.concatenate(factor, axis=1)
    else:
        factor = gain_rows[...]
    scaled = values * factor
    row = lax.broadcasted_iota(jnp.int32, (LANES, 2 * LANES), 0)
    column = lax.broadcasted_iota(jnp.int32, (LANES, 2 * LANES), 1)
    low = scaled.astype(bf16)
    apart = []
    for index in range(2):
        place = (column == 2 * row + index).astype(f32).astype(bf16)
        apart.append(
            jnp.concatenate(
                [
                    jnp.dot(low[:, at : at + LANES], place[: min(LANES, local_d), : 2 * min(LANES, local_d)], preferred_element_type=f32)
                    for at in range(0, local_d, LANES)
                ],
                axis=1,
            )
        )
    apart = jnp.concatenate(apart, axis=0).astype(bf16)

    high = squares.astype(bf16).astype(f32)
    step = lax.dot_general(low, ws[...], NT, preferred_element_type=f32)
    step_rows[...] = jnp.zeros_like(step_rows)
    step_rows[:, :heads] = pick(step, tp, n_tp, heads)
    step = step_rows[...]
    lane = lax.broadcasted_iota(jnp.int32, step.shape, 1)
    step = jnp.where(lane == heads, high, jnp.where(lane == heads + 1, squares - high, step))

    def put(at, part):
        for k in range(n_kv):
            piece = part[k * rows : (k + 1) * rows].astype(bf16)
            outs[k][:, at : at + part.shape[1]] = piece

    put(2 * width + 2 * bc, step)
    maps.wait()
    group = 2 * LANES if bc % (2 * LANES) == 0 else LANES
    for at in range(0, bc, group):
        block = [
            pairs[:, :, lane : lane + LANES].reshape(2 * local_d, LANES)
            for lane in range(at, at + group, LANES)
        ]
        both = jnp.dot(apart, jnp.concatenate(block, axis=1), preferred_element_type=f32)
        put(width + at, both[: n_kv * rows])
        put(width + bc + at, both[n_kv * rows :])
    count = len(plan) // 2
    for copy, at, here in plan[:count]:
        copy.wait()
        put(at, jnp.dot(low, wide[:, here], preferred_element_type=f32))
    for copy, at, here in plan[count:]:
        copy.wait()
        put(at, jnp.dot(low, wide[:, here], preferred_element_type=f32))


def state_kernel(
    n_tp,
    acc,
    state,
    past_x,
    past_maps,
    past_logs,
    heads_window,
    maps_window,
    head_taps,
    map_taps,
    bias,
    speed,
    direct,
    norm_gain,
    new_state,
    state_low,
    tail_x,
    tail_maps,
    conv_tail,
    taps,
    vectors,
    small,
    gain_rows,
):
    tp = lax.axis_index("tp")
    own, heads = state.shape[:2]
    props, width = past_x.shape[1:]
    bc = past_maps.shape[2]
    groups = bc // STATE
    per_group = heads // groups
    group_width = per_group * HEAD_DIM
    keep = CONV - 1

    head_cols = pl.ds(pl.multiple_of(tp * width, LANES), width)
    map_cols = pl.ds(pl.multiple_of(tp * bc, LANES), bc)
    weight_x = head_taps[:, head_cols].astype(f32)
    taps[:, :width] = weight_x
    weight_b, weight_c = [], []
    for k in range(CONV):
        pair = map_taps[k, :, map_cols].astype(f32)
        weight_b.append(pair[0:1])
        weight_c.append(pair[1:2])
        taps[k : k + 1, width : width + bc] = pair[0:1]
        taps[k : k + 1, width + bc :] = pair[1:2]
    direct_half = pick(direct[...], tp, n_tp, heads)
    vectors[0:1, :] = spread(direct_half, heads)
    gain_rows[...] = norm_gain[...].astype(f32)
    per_row = width // LANES
    for j in range(per_row):
        vectors[1:2, j * LANES : (j + 1) * LANES] = gain_rows[pl.ds(tp * per_row + j, 1), :]
    small[0:1, :heads] = pick(bias[...], tp, n_tp, heads)
    small[1:2, :heads] = pick(speed[...], tp, n_tp, heads)

    for s in range(own):
        a = acc[s]
        xs, bs, cs = [], [], []
        for k in range(keep):
            row = heads_window[a + k].astype(f32)
            xs.append(row[s : s + 1])
            pair = maps_window[s, a + k]
            tail_maps[s, k] = pair
            pair = pair.astype(f32)
            bs.append(pair[0:1])
            cs.append(pair[1:2])
        for k in range(keep):
            tail_x[k, s : s + 1, :] = xs[k].astype(bf16)
        for at, weights, rows in (
            (0, [weight_x[k : k + 1] for k in range(CONV)], xs),
            (width, weight_b, bs),
            (width + bc, weight_c, cs),
        ):
            size = rows[0].shape[1]
            for t in range(props):
                total = jnp.zeros((1, size), f32)
                for k in range(CONV):
                    if t + k < keep:
                        total = total + weights[k] * rows[t + k]
                conv_tail[s * props + t : s * props + t + 1, at : at + size] = total

        logs = past_logs[s]
        after = jnp.zeros((1, heads), f32)
        coefficients = [None] * props
        for j in reversed(range(props)):
            coefficients[j] = jnp.where(j < a, jnp.exp(after), 0.0)
            after = after + jnp.where(j < a, logs[j : j + 1], 0.0)
        factor = jnp.exp(after)
        coefficient = spread(jnp.concatenate(coefficients, axis=0), heads)
        scaled = past_x[s].astype(f32) * coefficient
        high = scaled.astype(bf16).astype(f32)
        left = jnp.concatenate([high, scaled - high], axis=0)
        maps = past_maps[s].astype(f32)
        maps = jnp.concatenate([maps, maps], axis=0).astype(bf16)
        for g in range(groups):
            block = left[:, g * group_width : (g + 1) * group_width]
            update = lax.dot_general(
                block.astype(bf16),
                maps[:, g * STATE : (g + 1) * STATE],
                TN,
                preferred_element_type=f32,
            )
            for i in range(per_group):
                h = g * per_group + i
                value = state[s, h] * factor[:, h : h + 1]
                value = value + update[i * HEAD_DIM : (i + 1) * HEAD_DIM]
                new_state[s, h] = value
                state_low[s, h * HEAD_DIM : (h + 1) * HEAD_DIM, :] = value.astype(bf16)


def mixer_kernel(
    n_features,
    n_blocks,
    decay_total,
    state_low,
    conv_tail,
    taps,
    vectors,
    small,
    *rest,
):
    blocks = rest[:n_blocks]
    normed, raw_out, weighted_out, maps_out, logs_out = rest[n_blocks:]
    own, _, heads = decay_total.shape
    rows, width = weighted_out.shape
    props = rows // own
    bc = (conv_tail.shape[1] - width) // 2
    groups = bc // STATE
    group_width = width // groups
    total = None
    for block in blocks:
        for piece in [block[...]] if len(block.shape) == 2 else [block[i] for i in range(block.shape[0])]:
            piece = piece.astype(f32)
            total = piece if total is None else total + piece
    conv_width = width + 2 * bc
    tail = total[:, conv_width + width :]
    squares = tail[:, heads : heads + 1] + tail[:, heads + 1 : heads + 2]
    inv_rms = lax.rsqrt(squares / n_features + eps)
    raw = (total[:, :conv_width] * inv_rms).astype(bf16)
    raw_out[...] = raw
    raw = raw.astype(f32)
    gate = total[:, conv_width : conv_width + width] * inv_rms

    step_pre = tail[:, :heads] * inv_rms + small[0:1, :heads]
    step = jnp.maximum(step_pre, 0.0) + jnp.log1p(jnp.exp(-jnp.abs(step_pre)))
    totals = jnp.concatenate([decay_total[s] for s in range(own)], axis=0)
    logs = totals - small[1:2, :heads] * step
    logs_out[...] = logs
    step = spread(step, heads)
    decay = spread(jnp.exp(logs), heads)

    def turn(value, d):
        return pltpu.roll(value, d, 0)

    def since(size):
        return lax.rem(lax.broadcasted_iota(jnp.int32, (rows, size), 0), props)

    pos = since(conv_width)
    conv = conv_tail[...] + taps[CONV - 1 : CONV] * raw
    for d in range(1, CONV):
        conv = conv + jnp.where(pos >= d, taps[CONV - 1 - d : CONV - d] * turn(raw, d), 0.0)
    conv = silu(conv)
    x_conv = conv[:, :width]
    b_conv = conv[:, width : width + bc]
    c_conv = conv[:, width + bc :]
    maps_out[...] = b_conv
    weighted = step * x_conv
    weighted_out[...] = weighted

    pos = since(width)
    c_low = c_conv.astype(bf16)
    row_seq = lax.broadcasted_iota(jnp.int32, (rows, group_width), 0) // props
    from_state = []
    for g in range(groups):
        left = c_low[:, g * STATE : (g + 1) * STATE]
        out = None
        for s in range(own):
            part = lax.dot_general(
                left,
                state_low[s, g * group_width : (g + 1) * group_width, :],
                NT,
                preferred_element_type=f32,
            )
            out = part if out is None else jnp.where(row_seq >= s, part, out)
        from_state.append(out)
    from_state = jnp.concatenate(from_state, axis=1)

    span = decay
    to_start = decay
    heads_out = vectors[0:1] * x_conv
    for d in range(props):
        product = c_conv * (b_conv if d == 0 else turn(b_conv, d))
        scores = jnp.concatenate(
            [
                jnp.broadcast_to(
                    jnp.sum(product[:, g * STATE : (g + 1) * STATE], axis=1, keepdims=True),
                    (rows, group_width),
                )
                for g in range(groups)
            ],
            axis=1,
        )
        if d == 0:
            heads_out = heads_out + scores * weighted
        else:
            term = scores * span * turn(weighted, d)
            heads_out = heads_out + jnp.where(pos >= d, term, 0.0)
            span = span * turn(decay, d)
            to_start = jnp.where(pos >= d, span, to_start)
    heads_out = heads_out + to_start * from_state
    gated = heads_out * silu(gate)
    for g in range(groups):
        lanes = slice(g * group_width, (g + 1) * group_width)
        part = gated[:, lanes]
        mean = jnp.sum(part * part, axis=1, keepdims=True) / group_width
        normed[:, lanes] = (part * lax.rsqrt(mean + eps) * vectors[1:2, lanes]).astype(bf16)


def outputs_kernel(
    raw, weighted, maps, logs, tail_x, tail_maps, head_input, input_maps, log_decays, heads_window, maps_window
):
    own, props, width = head_input.shape
    bc = input_maps.shape[2]
    keep = CONV - 1
    heads_window[:keep] = tail_x[...]
    rows = raw[...].astype(f32)
    weighted, maps, logs = weighted[...], maps[...], logs[...]
    for s in range(own):
        mine = slice(s * props, (s + 1) * props)
        head_input[s] = weighted[mine].astype(bf16)
        input_maps[s] = maps[mine].astype(bf16)
        log_decays[s] = logs[mine]
        maps_window[s, :keep] = tail_maps[s]
        for t in range(props):
            r = s * props + t
            pair = [rows[r : r + 1, width : width + bc], rows[r : r + 1, width + bc :]]
            maps_window[s, keep + t] = jnp.concatenate(pair, axis=0).astype(bf16)
    for t in range(props):
        both = [rows[s * props + t : s * props + t + 1, :width] for s in range(own)]
        heads_window[keep + t] = jnp.concatenate(both, axis=0).astype(bf16)


def mix_kernel(n_kv, weight, *rest):
    blocks, out = rest[:-1], rest[-1]
    kv = lax.axis_index("kv")
    _, props, _ = out.shape
    pieces = []
    for block in blocks:
        pieces += [block[...]] if len(block.shape) == 2 else [block[i] for i in range(block.shape[0])]
    rows = pieces[0].shape[0]
    own = rows // props
    left = jnp.concatenate([piece.astype(f32) for piece in pieces], axis=0).astype(bf16)
    part = jnp.dot(left, weight[...], preferred_element_type=f32)
    for k in range(n_kv):
        start = peer(kv, k, n_kv, back=True) * own
        for s in range(own):
            at = k * rows + s * props
            out[start + s] = part[at : at + props].astype(bf16)


def local(
    tokens,
    input_norm_gain,
    head_input_weight,
    output_gate_weight,
    state_maps_weight,
    step_size_weight,
    step_size_bias,
    head_decay_speed,
    proposal_decay_total,
    head_input_kernel,
    state_maps_kernel,
    head_direct_gain,
    grouped_norm_gain,
    output_weight,
    prior_state_value,
    previous_head_input,
    previous_input_maps,
    previous_log_decays,
    prior_heads_window,
    prior_maps_window,
    accepted,
):
    n_kv, n_tp = lax.axis_size("kv"), lax.axis_size("tp")
    kv = lax.axis_index("kv")
    seqs, props, local_d = tokens.shape
    heads = step_size_weight.shape[1] // n_tp
    width = head_input_weight.shape[1]
    bc = state_maps_weight.shape[2]
    own = prior_state_value.shape[0]
    rows = own * props
    conv_width = width + 2 * bc
    packed = conv_width + width + LANES
    sds = jax.ShapeDtypeStruct
    vmem = pl.BlockSpec(memory_space=pltpu.VMEM)

    if local_d % LANES == 0:
        gain = input_norm_gain.reshape(-1, LANES)
        step_weight = step_size_weight.T
    else:
        gain = lax.dynamic_slice_in_dim(input_norm_gain, kv * local_d, local_d, 0)
        gain = gain.reshape(1, local_d)
        step_weight = lax.dynamic_slice_in_dim(step_size_weight.T, kv * local_d, local_d, 1)
    chunk = width
    n_copies = 3 + 2 * (width // chunk) + 1
    hbm = pl.BlockSpec(memory_space=pltpu.HBM)
    sent = pl.pallas_call(
        functools.partial(project_kernel, n_kv, n_tp, chunk),
        out_shape=[sds((rows, packed), bf16)] * n_kv,
        in_specs=[hbm] * 6,
        scratch_shapes=[
            pltpu.VMEM(tokens.shape, bf16),
            pltpu.VMEM(gain.shape, bf16),
            pltpu.VMEM(gain.shape, f32),
            pltpu.VMEM((step_weight.shape[0], local_d), bf16),
            pltpu.VMEM((n_kv * rows, LANES), f32),
            pltpu.VMEM((local_d, 2 * width), bf16),
            pltpu.VMEM((local_d, 2, bc), bf16),
            pltpu.SemaphoreType.DMA((n_copies,)),
        ],
        compiler_params=params(12),
        name="project",
    )(
        *(
            pltpu.with_memory_space_constraint(array, pltpu.HBM)
            for array in (
                tokens,
                gain,
                head_input_weight,
                state_maps_weight,
                output_gate_weight,
                step_weight,
            )
        )
    )
    if n_kv <= DIRECT:
        got = [permute(sent[k], "kv", k, n_kv) for k in (2, 1, 3)]
        got = [sent[0]] + got
    else:
        got = [lax.all_to_all(jnp.stack(sent), "kv", 0, 0)]

    (
        accepted_state,
        state_low,
        tail_x,
        tail_maps,
        conv_tail,
        taps,
        vectors,
        small,
    ) = pl.pallas_call(
        functools.partial(state_kernel, n_tp),
        out_shape=[
            sds(prior_state_value.shape, f32),
            sds((own, width, STATE), bf16),
            sds((CONV - 1, own, width), bf16),
            sds((own, CONV - 1, 2, bc), bf16),
            sds((rows, conv_width), f32),
            sds((CONV, conv_width), f32),
            sds((2, width), f32),
            sds((2, LANES), f32),
        ],
        in_specs=[pl.BlockSpec(memory_space=pltpu.SMEM)] + [vmem] * 12,
        scratch_shapes=[pltpu.VMEM((n_tp * width // LANES, LANES), f32)],
        compiler_params=params(12),
        name="state",
    )(
        accepted,
        prior_state_value,
        previous_head_input,
        previous_input_maps,
        previous_log_decays,
        jnp.transpose(prior_heads_window, (1, 0, 2)),
        prior_maps_window,
        head_input_kernel,
        state_maps_kernel,
        step_size_bias.reshape(1, -1),
        head_decay_speed.reshape(1, -1),
        head_direct_gain.reshape(1, -1),
        grouped_norm_gain.reshape(-1, LANES),
    )

    normed, raw, weighted, maps, logs = pl.pallas_call(
        functools.partial(mixer_kernel, local_d * n_kv, len(got)),
        out_shape=[
            sds((rows, width), bf16),
            sds((rows, conv_width), bf16),
            sds((rows, width), f32),
            sds((rows, bc), f32),
            sds((rows, heads), f32),
        ],
        compiler_params=params(8),
        name="mixer",
    )(proposal_decay_total, state_low, conv_tail, taps, vectors, small, *got)

    if n_kv <= DIRECT:
        gd = {k: permute(normed, "kv", k, n_kv) for k in (3, 2, 1)}
        gathered = [normed] + [gd[k] for k in sorted(gd)]
    else:
        gathered = [lax.all_gather(normed, "kv")]

    head_input, input_maps, log_decays, heads_window, maps_window = pl.pallas_call(
        outputs_kernel,
        out_shape=[
            sds((own, props, width), bf16),
            sds((own, props, bc), bf16),
            sds((own, props, heads), f32),
            sds((CONV - 1 + props, own, width), bf16),
            sds((own, CONV - 1 + props, 2, bc), bf16),
        ],
        compiler_params=params(8),
        name="outputs",
    )(raw, weighted, maps, logs, tail_x, tail_maps)

    part = pl.pallas_call(
        functools.partial(mix_kernel, n_kv),
        out_shape=sds((seqs, props, local_d), bf16),
        compiler_params=params(8),
        name="mix",
    )(output_weight, *gathered)
    total = part.astype(f32)
    for k in range(1, n_tp):
        total = total + permute(part, "tp", k, n_tp).astype(f32)
    return (
        total.astype(bf16),
        accepted_state,
        head_input,
        input_maps,
        log_decays,
        jnp.transpose(heads_window, (1, 0, 2)),
        maps_window,
    )


def solution(mesh):
    return jax.shard_map(
        local,
        mesh=mesh,
        in_specs=(
            P("dp", None, "kv"),
            P(),
            P("kv", "tp"),
            P("kv", "tp"),
            P("kv", None, "tp"),
            P(),
            P(),
            P(),
            P(("dp", "kv"), None, "tp"),
            P(),
            P(),
            P(),
            P(),
            P("tp", "kv"),
            P(("dp", "kv"), "tp", None, None),
            P(("dp", "kv"), None, "tp"),
            P(("dp", "kv"), None, "tp"),
            P(("dp", "kv"), None, "tp"),
            P(("dp", "kv"), None, "tp"),
            P(("dp", "kv"), None, None, "tp"),
            P(("dp", "kv")),
        ),
        out_specs=(
            P("dp", None, "kv"),
            P(("dp", "kv"), "tp", None, None),
            P(("dp", "kv"), None, "tp"),
            P(("dp", "kv"), None, "tp"),
            P(("dp", "kv"), None, "tp"),
            P(("dp", "kv"), None, "tp"),
            P(("dp", "kv"), None, None, "tp"),
        ),
        check_vma=False,
    )
```

```python
import functools

import jax
import jax.numpy as jnp
from jax import lax
from jax.experimental import pallas as pl
from jax.experimental.pallas import tpu as pltpu
from jax.sharding import PartitionSpec as P

HEAD_DIM = 64
STATE = 128
CONV = 4
LANES = 128
DIRECT = 8

eps = 1e-06
f32 = jnp.float32
bf16 = jnp.bfloat16

NT = (((1,), (1,)), ((), ()))
TN = (((0,), (0,)), ((), ()))


def params(mib):
    return pltpu.CompilerParams(vmem_limit_bytes=mib << 20)


def peer(me, k, n, ring, back=False):
    if n > DIRECT:
        return k
    if ring or n & (n - 1):
        at = me + (n - k if back else k)
        return at % n if isinstance(me, int) else lax.rem(at, n)
    return me ^ k


def permute(array, axis, k, n, ring=False):
    return lax.ppermute(array, axis, [(i, peer(i, k, n, ring)) for i in range(n)])


def pick(rows, index, count, width):
    out = rows[:, :width]
    for block in range(1, count):
        out = jnp.where(index == block, rows[:, block * width : (block + 1) * width], out)
    return out


def spread(values, heads):
    rows = values.shape[0]
    per = LANES // HEAD_DIM
    lane = lax.broadcasted_iota(jnp.int32, (rows, LANES), 1)
    tiles = []
    for first in range(0, heads, per):
        tile = jnp.broadcast_to(values[:, first : first + 1], (rows, LANES))
        for j in range(1, per):
            other = jnp.broadcast_to(values[:, first + j : first + j + 1], (rows, LANES))
            tile = jnp.where(lane >= j * HEAD_DIM, other, tile)
        tiles.append(tile)
    return jnp.concatenate(tiles, axis=1)


def silu(x):
    return x * (1.0 / (1.0 + jnp.exp(-x)))


def project_kernel(n_kv, n_tp, chunk, tok_hbm, gain_hbm, wx, wm, wg, ws_hbm, *rest):
    outs = rest[:n_kv]
    tok, gain, gain_rows, ws, step_rows, wide, pairs, sems = rest[n_kv:]
    kv, tp = lax.axis_index("kv"), lax.axis_index("tp")
    seqs, props, local_d = tok.shape
    own = seqs // n_kv
    rows = own * props
    width, bc = wx.shape[1], wm.shape[2]
    heads = ws.shape[0] // n_tp
    aligned = local_d % LANES == 0

    copies = []

    def fetch(source, target):
        copy = pltpu.make_async_copy(source, target, sems.at[len(copies)])
        copy.start()
        copies.append(copy)
        return copy

    small = [fetch(tok_hbm, tok), fetch(gain_hbm, gain)]
    columns = pl.ds(pl.multiple_of(kv * local_d, LANES), local_d) if aligned else slice(None)
    small.append(fetch(ws_hbm.at[:, columns], ws))
    maps = fetch(wm, pairs)
    plan = []
    for at in range(0, width, chunk):
        here = slice(at, at + chunk)
        plan.append((fetch(wx.at[:, here], wide.at[:, here]), at, here))
    for at in range(0, width, chunk):
        here = slice(width + at, width + at + chunk)
        plan.append((fetch(wg.at[:, at : at + chunk], wide.at[:, here]), width + 2 * bc + at, here))

    for copy in small:
        copy.wait()
    parts = []
    for k in range(n_kv):
        start = peer(kv, k, n_kv, False) * own
        for s in range(own):
            parts.append(tok[start + s].astype(f32))
    values = jnp.concatenate(parts, axis=0)
    squares = jnp.sum(values * values, axis=1, keepdims=True)
    gain_rows[...] = gain[...].astype(f32)
    if aligned:
        per = local_d // LANES
        factor = [gain_rows[pl.ds(kv * per + j, 1), :] for j in range(per)]
        factor = jnp.concatenate(factor, axis=1)
    else:
        factor = gain_rows[...]
    scaled = values * factor
    row = lax.broadcasted_iota(jnp.int32, (LANES, 2 * LANES), 0)
    column = lax.broadcasted_iota(jnp.int32, (LANES, 2 * LANES), 1)
    low = scaled.astype(bf16)
    apart = []
    for index in range(2):
        place = (column == 2 * row + index).astype(f32).astype(bf16)
        apart.append(
            jnp.concatenate(
                [
                    jnp.dot(low[:, at : at + LANES], place[: min(LANES, local_d), : 2 * min(LANES, local_d)], preferred_element_type=f32)
                    for at in range(0, local_d, LANES)
                ],
                axis=1,
            )
        )
    apart = jnp.concatenate(apart, axis=0).astype(bf16)

    high = squares.astype(bf16).astype(f32)
    step = lax.dot_general(low, ws[...], NT, preferred_element_type=f32)
    step_rows[...] = jnp.zeros_like(step_rows)
    step_rows[:, :heads] = pick(step, tp, n_tp, heads)
    step = step_rows[...]
    lane = lax.broadcasted_iota(jnp.int32, step.shape, 1)
    step = jnp.where(lane == heads, high, jnp.where(lane == heads + 1, squares - high, step))

    def put(at, part):
        for k in range(n_kv):
            piece = part[k * rows : (k + 1) * rows].astype(bf16)
            outs[k][:, at : at + part.shape[1]] = piece

    put(2 * width + 2 * bc, step)
    maps.wait()
    group = 2 * LANES if bc % (2 * LANES) == 0 else LANES
    for at in range(0, bc, group):
        block = [
            pairs[:, :, lane : lane + LANES].reshape(2 * local_d, LANES)
            for lane in range(at, at + group, LANES)
        ]
        both = jnp.dot(apart, jnp.concatenate(block, axis=1), preferred_element_type=f32)
        put(width + at, both[: n_kv * rows])
        put(width + bc + at, both[n_kv * rows :])
    count = len(plan) // 2
    for copy, at, here in plan[:count]:
        copy.wait()
        put(at, jnp.dot(low, wide[:, here], preferred_element_type=f32))
    for copy, at, here in plan[count:]:
        copy.wait()
        put(at, jnp.dot(low, wide[:, here], preferred_element_type=f32))


def state_kernel(
    n_tp,
    acc,
    state,
    past_x,
    past_maps,
    past_logs,
    heads_window,
    maps_window,
    head_taps,
    map_taps,
    bias,
    speed,
    direct,
    norm_gain,
    new_state,
    state_low,
    tail_x,
    tail_maps,
    conv_tail,
    taps,
    vectors,
    small,
    gain_rows,
):
    tp = lax.axis_index("tp")
    own, heads = state.shape[:2]
    props, width = past_x.shape[1:]
    bc = past_maps.shape[2]
    groups = bc // STATE
    per_group = heads // groups
    group_width = per_group * HEAD_DIM
    keep = CONV - 1

    head_cols = pl.ds(pl.multiple_of(tp * width, LANES), width)
    map_cols = pl.ds(pl.multiple_of(tp * bc, LANES), bc)
    weight_x = head_taps[:, head_cols].astype(f32)
    taps[:, :width] = weight_x
    weight_b, weight_c = [], []
    for k in range(CONV):
        pair = map_taps[k, :, map_cols].astype(f32)
        weight_b.append(pair[0:1])
        weight_c.append(pair[1:2])
        taps[k : k + 1, width : width + bc] = pair[0:1]
        taps[k : k + 1, width + bc :] = pair[1:2]
    direct_half = pick(direct[...], tp, n_tp, heads)
    vectors[0:1, :] = spread(direct_half, heads)
    gain_rows[...] = norm_gain[...].astype(f32)
    per_row = width // LANES
    for j in range(per_row):
        vectors[1:2, j * LANES : (j + 1) * LANES] = gain_rows[pl.ds(tp * per_row + j, 1), :]
    small[0:1, :heads] = pick(bias[...], tp, n_tp, heads)
    small[1:2, :heads] = pick(speed[...], tp, n_tp, heads)

    for s in range(own):
        a = acc[s]
        xs, bs, cs = [], [], []
        for k in range(keep):
            row = heads_window[a + k].astype(f32)
            xs.append(row[s : s + 1])
            pair = maps_window[s, a + k]
            tail_maps[s, k] = pair
            pair = pair.astype(f32)
            bs.append(pair[0:1])
            cs.append(pair[1:2])
        for k in range(keep):
            tail_x[k, s : s + 1, :] = xs[k].astype(bf16)
        for at, weights, rows in (
            (0, [weight_x[k : k + 1] for k in range(CONV)], xs),
            (width, weight_b, bs),
            (width + bc, weight_c, cs),
        ):
            size = rows[0].shape[1]
            for t in range(props):
                total = jnp.zeros((1, size), f32)
                for k in range(CONV):
                    if t + k < keep:
                        total = total + weights[k] * rows[t + k]
                conv_tail[s * props + t : s * props + t + 1, at : at + size] = total

        logs = past_logs[s]
        after = jnp.zeros((1, heads), f32)
        coefficients = [None] * props
        for j in reversed(range(props)):
            coefficients[j] = jnp.where(j < a, jnp.exp(after), 0.0)
            after = after + jnp.where(j < a, logs[j : j + 1], 0.0)
        factor = jnp.exp(after)
        coefficient = spread(jnp.concatenate(coefficients, axis=0), heads)
        scaled = past_x[s].astype(f32) * coefficient
        high = scaled.astype(bf16).astype(f32)
        left = jnp.concatenate([high, scaled - high], axis=0)
        maps = past_maps[s].astype(f32)
        maps = jnp.concatenate([maps, maps], axis=0).astype(bf16)
        for g in range(groups):
            block = left[:, g * group_width : (g + 1) * group_width]
            update = lax.dot_general(
                block.astype(bf16),
                maps[:, g * STATE : (g + 1) * STATE],
                TN,
                preferred_element_type=f32,
            )
            for i in range(per_group):
                h = g * per_group + i
                value = state[s, h] * factor[:, h : h + 1]
                value = value + update[i * HEAD_DIM : (i + 1) * HEAD_DIM]
                new_state[s, h] = value
                state_low[s, h * HEAD_DIM : (h + 1) * HEAD_DIM, :] = value.astype(bf16)


def mixer_kernel(
    n_features,
    n_blocks,
    decay_total,
    state_low,
    conv_tail,
    taps,
    vectors,
    small,
    *rest,
):
    blocks = rest[:n_blocks]
    normed, raw_out, weighted_out, maps_out, logs_out = rest[n_blocks:]
    own, _, heads = decay_total.shape
    rows, width = weighted_out.shape
    props = rows // own
    bc = (conv_tail.shape[1] - width) // 2
    groups = bc // STATE
    group_width = width // groups
    total = None
    for block in blocks:
        for piece in [block[...]] if len(block.shape) == 2 else [block[i] for i in range(block.shape[0])]:
            piece = piece.astype(f32)
            total = piece if total is None else total + piece
    conv_width = width + 2 * bc
    tail = total[:, conv_width + width :]
    squares = tail[:, heads : heads + 1] + tail[:, heads + 1 : heads + 2]
    inv_rms = lax.rsqrt(squares / n_features + eps)
    raw = (total[:, :conv_width] * inv_rms).astype(bf16)
    raw_out[...] = raw
    raw = raw.astype(f32)
    gate = total[:, conv_width : conv_width + width] * inv_rms

    step_pre = tail[:, :heads] * inv_rms + small[0:1, :heads]
    step = jnp.maximum(step_pre, 0.0) + jnp.log1p(jnp.exp(-jnp.abs(step_pre)))
    totals = jnp.concatenate([decay_total[s] for s in range(own)], axis=0)
    logs = totals - small[1:2, :heads] * step
    logs_out[...] = logs
    step = spread(step, heads)
    decay = spread(jnp.exp(logs), heads)

    def turn(value, d):
        return pltpu.roll(value, d, 0)

    def since(size):
        return lax.rem(lax.broadcasted_iota(jnp.int32, (rows, size), 0), props)

    pos = since(conv_width)
    conv = conv_tail[...] + taps[CONV - 1 : CONV] * raw
    for d in range(1, CONV):
        conv = conv + jnp.where(pos >= d, taps[CONV - 1 - d : CONV - d] * turn(raw, d), 0.0)
    conv = silu(conv)
    x_conv = conv[:, :width]
    b_conv = conv[:, width : width + bc]
    c_conv = conv[:, width + bc :]
    maps_out[...] = b_conv
    weighted = step * x_conv
    weighted_out[...] = weighted

    pos = since(width)
    c_low = c_conv.astype(bf16)
    row_seq = lax.broadcasted_iota(jnp.int32, (rows, group_width), 0) // props
    from_state = []
    for g in range(groups):
        left = c_low[:, g * STATE : (g + 1) * STATE]
        out = None
        for s in range(own):
            part = lax.dot_general(
                left,
                state_low[s, g * group_width : (g + 1) * group_width, :],
                NT,
                preferred_element_type=f32,
            )
            out = part if out is None else jnp.where(row_seq >= s, part, out)
        from_state.append(out)
    from_state = jnp.concatenate(from_state, axis=1)

    span = decay
    to_start = decay
    heads_out = vectors[0:1] * x_conv
    for d in range(props):
        product = c_conv * (b_conv if d == 0 else turn(b_conv, d))
        scores = jnp.concatenate(
            [
                jnp.broadcast_to(
                    jnp.sum(product[:, g * STATE : (g + 1) * STATE], axis=1, keepdims=True),
                    (rows, group_width),
                )
                for g in range(groups)
            ],
            axis=1,
        )
        if d == 0:
            heads_out = heads_out + scores * weighted
        else:
            term = scores * span * turn(weighted, d)
            heads_out = heads_out + jnp.where(pos >= d, term, 0.0)
            span = span * turn(decay, d)
            to_start = jnp.where(pos >= d, span, to_start)
    heads_out = heads_out + to_start * from_state
    gated = heads_out * silu(gate)
    for g in range(groups):
        lanes = slice(g * group_width, (g + 1) * group_width)
        part = gated[:, lanes]
        mean = jnp.sum(part * part, axis=1, keepdims=True) / group_width
        normed[:, lanes] = (part * lax.rsqrt(mean + eps) * vectors[1:2, lanes]).astype(bf16)


def outputs_kernel(
    raw, weighted, maps, logs, tail_x, tail_maps, head_input, input_maps, log_decays, heads_window, maps_window
):
    own, props, width = head_input.shape
    bc = input_maps.shape[2]
    keep = CONV - 1
    heads_window[:keep] = tail_x[...]
    rows = raw[...].astype(f32)
    weighted, maps, logs = weighted[...], maps[...], logs[...]
    for s in range(own):
        mine = slice(s * props, (s + 1) * props)
        head_input[s] = weighted[mine].astype(bf16)
        input_maps[s] = maps[mine].astype(bf16)
        log_decays[s] = logs[mine]
        maps_window[s, :keep] = tail_maps[s]
        for t in range(props):
            r = s * props + t
            pair = [rows[r : r + 1, width : width + bc], rows[r : r + 1, width + bc :]]
            maps_window[s, keep + t] = jnp.concatenate(pair, axis=0).astype(bf16)
    for t in range(props):
        both = [rows[s * props + t : s * props + t + 1, :width] for s in range(own)]
        heads_window[keep + t] = jnp.concatenate(both, axis=0).astype(bf16)


def mix_kernel(n_kv, order, weight, *rest):
    blocks, out = rest[:-1], rest[-1]
    kv = lax.axis_index("kv")
    _, props, _ = out.shape
    pieces = []
    for block in blocks:
        pieces += [block[...]] if len(block.shape) == 2 else [block[i] for i in range(block.shape[0])]
    rows = pieces[0].shape[0]
    own = rows // props
    left = jnp.concatenate([piece.astype(f32) for piece in pieces], axis=0).astype(bf16)
    part = jnp.dot(left, weight[...], preferred_element_type=f32)
    for i, k in enumerate(order):
        start = peer(kv, k, n_kv, True, back=True) * own
        for s in range(own):
            at = i * rows + s * props
            out[start + s] = part[at : at + props].astype(bf16)


def local(
    tokens,
    input_norm_gain,
    head_input_weight,
    output_gate_weight,
    state_maps_weight,
    step_size_weight,
    step_size_bias,
    head_decay_speed,
    proposal_decay_total,
    head_input_kernel,
    state_maps_kernel,
    head_direct_gain,
    grouped_norm_gain,
    output_weight,
    prior_state_value,
    previous_head_input,
    previous_input_maps,
    previous_log_decays,
    prior_heads_window,
    prior_maps_window,
    accepted,
):
    n_kv, n_tp = lax.axis_size("kv"), lax.axis_size("tp")
    kv = lax.axis_index("kv")
    seqs, props, local_d = tokens.shape
    heads = step_size_weight.shape[1] // n_tp
    width = head_input_weight.shape[1]
    bc = state_maps_weight.shape[2]
    own = prior_state_value.shape[0]
    rows = own * props
    conv_width = width + 2 * bc
    packed = conv_width + width + LANES
    sds = jax.ShapeDtypeStruct
    vmem = pl.BlockSpec(memory_space=pltpu.VMEM)

    if local_d % LANES == 0:
        gain = input_norm_gain.reshape(-1, LANES)
        step_weight = step_size_weight.T
    else:
        gain = lax.dynamic_slice_in_dim(input_norm_gain, kv * local_d, local_d, 0)
        gain = gain.reshape(1, local_d)
        step_weight = lax.dynamic_slice_in_dim(step_size_weight.T, kv * local_d, local_d, 1)
    chunk = width
    n_copies = 3 + 2 * (width // chunk) + 1
    hbm = pl.BlockSpec(memory_space=pltpu.HBM)
    sent = pl.pallas_call(
        functools.partial(project_kernel, n_kv, n_tp, chunk),
        out_shape=[sds((rows, packed), bf16)] * n_kv,
        in_specs=[hbm] * 6,
        scratch_shapes=[
            pltpu.VMEM(tokens.shape, bf16),
            pltpu.VMEM(gain.shape, bf16),
            pltpu.VMEM(gain.shape, f32),
            pltpu.VMEM((step_weight.shape[0], local_d), bf16),
            pltpu.VMEM((n_kv * rows, LANES), f32),
            pltpu.VMEM((local_d, 2 * width), bf16),
            pltpu.VMEM((local_d, 2, bc), bf16),
            pltpu.SemaphoreType.DMA((n_copies,)),
        ],
        compiler_params=params(12),
        name="project",
    )(
        *(
            pltpu.with_memory_space_constraint(array, pltpu.HBM)
            for array in (
                tokens,
                gain,
                head_input_weight,
                state_maps_weight,
                output_gate_weight,
                step_weight,
            )
        )
    )
    if n_kv <= DIRECT:
        order = sorted(range(1, n_kv), key=lambda k: (k % 2, k))
        got = [permute(sent[k], "kv", k, n_kv) for k in order]
        got = [sent[0]] + got
    else:
        got = [lax.all_to_all(jnp.stack(sent), "kv", 0, 0)]

    (
        accepted_state,
        state_low,
        tail_x,
        tail_maps,
        conv_tail,
        taps,
        vectors,
        small,
    ) = pl.pallas_call(
        functools.partial(state_kernel, n_tp),
        out_shape=[
            sds(prior_state_value.shape, f32),
            sds((own, width, STATE), bf16),
            sds((CONV - 1, own, width), bf16),
            sds((own, CONV - 1, 2, bc), bf16),
            sds((rows, conv_width), f32),
            sds((CONV, conv_width), f32),
            sds((2, width), f32),
            sds((2, LANES), f32),
        ],
        in_specs=[pl.BlockSpec(memory_space=pltpu.SMEM)] + [vmem] * 12,
        scratch_shapes=[pltpu.VMEM((n_tp * width // LANES, LANES), f32)],
        compiler_params=params(12),
        name="state",
    )(
        accepted,
        prior_state_value,
        previous_head_input,
        previous_input_maps,
        previous_log_decays,
        jnp.transpose(prior_heads_window, (1, 0, 2)),
        prior_maps_window,
        head_input_kernel,
        state_maps_kernel,
        step_size_bias.reshape(1, -1),
        head_decay_speed.reshape(1, -1),
        head_direct_gain.reshape(1, -1),
        grouped_norm_gain.reshape(-1, LANES),
    )

    normed, raw, weighted, maps, logs = pl.pallas_call(
        functools.partial(mixer_kernel, local_d * n_kv, len(got)),
        out_shape=[
            sds((rows, width), bf16),
            sds((rows, conv_width), bf16),
            sds((rows, width), f32),
            sds((rows, bc), f32),
            sds((rows, heads), f32),
        ],
        compiler_params=params(8),
        name="mixer",
    )(proposal_decay_total, state_low, conv_tail, taps, vectors, small, *got)

    if n_kv <= DIRECT:
        order = (0, *reversed(range(1, n_kv)))
        gathered = [normed] + [permute(normed, "kv", k, n_kv, True) for k in order[1:]]
    else:
        gathered = [lax.all_gather(normed, "kv")]
        order = tuple(range(n_kv))

    head_input, input_maps, log_decays, heads_window, maps_window = pl.pallas_call(
        outputs_kernel,
        out_shape=[
            sds((own, props, width), bf16),
            sds((own, props, bc), bf16),
            sds((own, props, heads), f32),
            sds((CONV - 1 + props, own, width), bf16),
            sds((own, CONV - 1 + props, 2, bc), bf16),
        ],
        compiler_params=params(8),
        name="outputs",
    )(raw, weighted, maps, logs, tail_x, tail_maps)

    part = pl.pallas_call(
        functools.partial(mix_kernel, n_kv, order),
        out_shape=sds((seqs, props, local_d), bf16),
        compiler_params=params(8),
        name="mix",
    )(output_weight, *gathered)
    total = part.astype(f32)
    for k in range(1, n_tp):
        total = total + permute(part, "tp", k, n_tp).astype(f32)
    return (
        total.astype(bf16),
        accepted_state,
        head_input,
        input_maps,
        log_decays,
        jnp.transpose(heads_window, (1, 0, 2)),
        maps_window,
    )


def solution(mesh):
    return jax.shard_map(
        local,
        mesh=mesh,
        in_specs=(
            P("dp", None, "kv"),
            P(),
            P("kv", "tp"),
            P("kv", "tp"),
            P("kv", None, "tp"),
            P(),
            P(),
            P(),
            P(("dp", "kv"), None, "tp"),
            P(),
            P(),
            P(),
            P(),
            P("tp", "kv"),
            P(("dp", "kv"), "tp", None, None),
            P(("dp", "kv"), None, "tp"),
            P(("dp", "kv"), None, "tp"),
            P(("dp", "kv"), None, "tp"),
            P(("dp", "kv"), None, "tp"),
            P(("dp", "kv"), None, None, "tp"),
            P(("dp", "kv")),
        ),
        out_specs=(
            P("dp", None, "kv"),
            P(("dp", "kv"), "tp", None, None),
            P(("dp", "kv"), None, "tp"),
            P(("dp", "kv"), None, "tp"),
            P(("dp", "kv"), None, "tp"),
            P(("dp", "kv"), None, "tp"),
            P(("dp", "kv"), None, None, "tp"),
        ),
        check_vma=False,
    )
```

```python
import functools

import jax
import jax.numpy as jnp
from jax import lax
from jax.experimental import pallas as pl
from jax.experimental.pallas import tpu as pltpu
from jax.sharding import PartitionSpec as P

HEAD_DIM = 64
STATE = 128
CONV = 4
LANES = 128
DIRECT = 8

eps = 1e-06
f32 = jnp.float32
bf16 = jnp.bfloat16

NT = (((1,), (1,)), ((), ()))
TN = (((0,), (0,)), ((), ()))


def params(mib):
    return pltpu.CompilerParams(vmem_limit_bytes=mib << 20)


def peer(me, k, n, ring, back=False):
    if n > DIRECT:
        return k
    if ring or n & (n - 1):
        at = me + (n - k if back else k)
        return at % n if isinstance(me, int) else lax.rem(at, n)
    return me ^ k


def permute(array, axis, k, n, ring=False):
    return lax.ppermute(array, axis, [(i, peer(i, k, n, ring)) for i in range(n)])


def pick(rows, index, count, width):
    out = rows[:, :width]
    for block in range(1, count):
        out = jnp.where(index == block, rows[:, block * width : (block + 1) * width], out)
    return out


def spread(values, heads):
    rows = values.shape[0]
    per = LANES // HEAD_DIM
    lane = lax.broadcasted_iota(jnp.int32, (rows, LANES), 1)
    tiles = []
    for first in range(0, heads, per):
        tile = jnp.broadcast_to(values[:, first : first + 1], (rows, LANES))
        for j in range(1, per):
            other = jnp.broadcast_to(values[:, first + j : first + j + 1], (rows, LANES))
            tile = jnp.where(lane >= j * HEAD_DIM, other, tile)
        tiles.append(tile)
    return jnp.concatenate(tiles, axis=1)


def silu(x):
    return x * (1.0 / (1.0 + jnp.exp(-x)))


def project_kernel(n_kv, n_tp, chunk, tok_hbm, gain_hbm, wx, wm, wg, ws_hbm, *rest):
    outs = rest[:n_kv]
    tok, gain, gain_rows, ws, step_rows, wide, pairs, sems = rest[n_kv:]
    kv, tp = lax.axis_index("kv"), lax.axis_index("tp")
    seqs, props, local_d = tok.shape
    own = seqs // n_kv
    rows = own * props
    width, bc = wx.shape[1], wm.shape[2]
    heads = ws.shape[0] // n_tp
    aligned = local_d % LANES == 0

    copies = []

    def fetch(source, target):
        copy = pltpu.make_async_copy(source, target, sems.at[len(copies)])
        copy.start()
        copies.append(copy)
        return copy

    small = [fetch(tok_hbm, tok), fetch(gain_hbm, gain)]
    columns = pl.ds(pl.multiple_of(kv * local_d, LANES), local_d) if aligned else slice(None)
    small.append(fetch(ws_hbm.at[:, columns], ws))
    maps = fetch(wm, pairs)
    plan = []
    for at in range(0, width, chunk):
        here = slice(at, at + chunk)
        plan.append((fetch(wx.at[:, here], wide.at[:, here]), at, here))
    for at in range(0, width, chunk):
        here = slice(width + at, width + at + chunk)
        plan.append((fetch(wg.at[:, at : at + chunk], wide.at[:, here]), width + 2 * bc + at, here))

    for copy in small:
        copy.wait()
    parts = []
    for k in range(n_kv):
        start = peer(kv, k, n_kv, False) * own
        for s in range(own):
            parts.append(tok[start + s].astype(f32))
    values = jnp.concatenate(parts, axis=0)
    squares = jnp.sum(values * values, axis=1, keepdims=True)
    gain_rows[...] = gain[...].astype(f32)
    if aligned:
        per = local_d // LANES
        factor = [gain_rows[pl.ds(kv * per + j, 1), :] for j in range(per)]
        factor = jnp.concatenate(factor, axis=1)
    else:
        factor = gain_rows[...]
    scaled = values * factor
    row = lax.broadcasted_iota(jnp.int32, (LANES, 2 * LANES), 0)
    column = lax.broadcasted_iota(jnp.int32, (LANES, 2 * LANES), 1)
    low = scaled.astype(bf16)
    apart = []
    for index in range(2):
        place = (column == 2 * row + index).astype(f32).astype(bf16)
        apart.append(
            jnp.concatenate(
                [
                    jnp.dot(low[:, at : at + LANES], place[: min(LANES, local_d), : 2 * min(LANES, local_d)], preferred_element_type=f32)
                    for at in range(0, local_d, LANES)
                ],
                axis=1,
            )
        )
    apart = jnp.concatenate(apart, axis=0).astype(bf16)

    high = squares.astype(bf16).astype(f32)
    step = lax.dot_general(low, ws[...], NT, preferred_element_type=f32)
    step_rows[...] = jnp.zeros_like(step_rows)
    step_rows[:, :heads] = pick(step, tp, n_tp, heads)
    step = step_rows[...]
    lane = lax.broadcasted_iota(jnp.int32, step.shape, 1)
    step = jnp.where(lane == heads, high, jnp.where(lane == heads + 1, squares - high, step))

    def put(at, part):
        for k in range(n_kv):
            piece = part[k * rows : (k + 1) * rows].astype(bf16)
            outs[k][:, at : at + part.shape[1]] = piece

    put(2 * width + 2 * bc, step)
    maps.wait()
    group = 2 * LANES if bc % (2 * LANES) == 0 else LANES
    for at in range(0, bc, group):
        block = [
            pairs[:, :, lane : lane + LANES].reshape(2 * local_d, LANES)
            for lane in range(at, at + group, LANES)
        ]
        both = jnp.dot(apart, jnp.concatenate(block, axis=1), preferred_element_type=f32)
        put(width + at, both[: n_kv * rows])
        put(width + bc + at, both[n_kv * rows :])
    count = len(plan) // 2
    for copy, at, here in plan[:count]:
        copy.wait()
        put(at, jnp.dot(low, wide[:, here], preferred_element_type=f32))
    for copy, at, here in plan[count:]:
        copy.wait()
        put(at, jnp.dot(low, wide[:, here], preferred_element_type=f32))


def state_kernel(
    n_tp,
    arrive,
    leave,
    acc,
    state,
    past_x,
    past_maps,
    past_logs,
    heads_window,
    maps_window,
    head_taps,
    map_taps,
    bias,
    speed,
    direct,
    norm_gain,
    state_low,
    tail_x,
    tail_maps,
    conv_tail,
    taps,
    vectors,
    small,
    gain_rows,
):
    tp = lax.axis_index("tp")
    own, heads = state.shape[:2]
    props, width = past_x.shape[1:]
    bc = past_maps.shape[2]
    groups = bc // STATE
    per_group = heads // groups
    group_width = per_group * HEAD_DIM
    keep = CONV - 1

    head_cols = pl.ds(pl.multiple_of(tp * width, LANES), width)
    map_cols = pl.ds(pl.multiple_of(tp * bc, LANES), bc)
    weight_x = head_taps[:, head_cols].astype(f32)
    taps[:, :width] = weight_x
    weight_b, weight_c = [], []
    for k in range(CONV):
        pair = map_taps[k, :, map_cols].astype(f32)
        weight_b.append(pair[0:1])
        weight_c.append(pair[1:2])
        taps[k : k + 1, width : width + bc] = pair[0:1]
        taps[k : k + 1, width + bc :] = pair[1:2]
    direct_half = pick(direct[...], tp, n_tp, heads)
    vectors[0:1, :] = spread(direct_half, heads)
    gain_rows[...] = norm_gain[...].astype(f32)
    per_row = width // LANES
    for j in range(per_row):
        vectors[1:2, j * LANES : (j + 1) * LANES] = gain_rows[pl.ds(tp * per_row + j, 1), :]
    small[0:1, :heads] = pick(bias[...], tp, n_tp, heads)
    small[1:2, :heads] = pick(speed[...], tp, n_tp, heads)

    for s in range(own):
        a = acc[s]
        xs, bs, cs = [], [], []
        for k in range(keep):
            row = heads_window[a + k].astype(f32)
            xs.append(row[s : s + 1])
            pair = maps_window[s, a + k]
            tail_maps[s, k] = pair
            pair = pair.astype(f32)
            bs.append(pair[0:1])
            cs.append(pair[1:2])
        for k in range(keep):
            tail_x[k, s : s + 1, :] = xs[k].astype(bf16)
        for at, weights, rows in (
            (0, [weight_x[k : k + 1] for k in range(CONV)], xs),
            (width, weight_b, bs),
            (width + bc, weight_c, cs),
        ):
            size = rows[0].shape[1]
            for t in range(props):
                total = jnp.zeros((1, size), f32)
                for k in range(CONV):
                    if t + k < keep:
                        total = total + weights[k] * rows[t + k]
                conv_tail[s * props + t : s * props + t + 1, at : at + size] = total

        logs = past_logs[s]
        after = jnp.zeros((1, heads), f32)
        coefficients = [None] * props
        for j in reversed(range(props)):
            coefficients[j] = jnp.where(j < a, jnp.exp(after), 0.0)
            after = after + jnp.where(j < a, logs[j : j + 1], 0.0)
        factor = jnp.exp(after)
        arrive(s)
        coefficient = spread(jnp.concatenate(coefficients, axis=0), heads)
        scaled = past_x[s].astype(f32) * coefficient
        high = scaled.astype(bf16).astype(f32)
        left = jnp.concatenate([high, scaled - high], axis=0)
        maps = past_maps[s].astype(f32)
        maps = jnp.concatenate([maps, maps], axis=0).astype(bf16)
        for g in range(groups):
            block = left[:, g * group_width : (g + 1) * group_width]
            update = lax.dot_general(
                block.astype(bf16),
                maps[:, g * STATE : (g + 1) * STATE],
                TN,
                preferred_element_type=f32,
            )
            for i in range(per_group):
                h = g * per_group + i
                value = state[s, h] * factor[:, h : h + 1]
                value = value + update[i * HEAD_DIM : (i + 1) * HEAD_DIM]
                state[s, h] = value
                state_low[s, h * HEAD_DIM : (h + 1) * HEAD_DIM, :] = value.astype(bf16)
        leave(s)


def fetched_state_kernel(n_tp, acc, state_hbm, *rest):
    sources, new_state, outs, rest = rest[:11], rest[11], rest[12:19], rest[19:]
    gain_rows, state, targets, sems, state_sems = rest[0], rest[1], rest[2:13], rest[13], rest[14]
    own = state.shape[0]
    small = [
        pltpu.make_async_copy(source, target, sems.at[i])
        for i, (source, target) in enumerate(zip(sources, targets, strict=True))
    ]
    inward = [
        pltpu.make_async_copy(state_hbm.at[s], state.at[s], state_sems.at[0, s])
        for s in range(own)
    ]
    outward = [
        pltpu.make_async_copy(state.at[s], new_state.at[s], state_sems.at[1, s])
        for s in range(own)
    ]
    for copy in small + inward:
        copy.start()
    for copy in small:
        copy.wait()
    state_kernel(
        n_tp,
        lambda s: inward[s].wait(),
        lambda s: outward[s].start(),
        acc,
        state,
        *targets,
        *outs,
        gain_rows,
    )
    for copy in outward:
        copy.wait()


def mixer_kernel(
    n_features,
    n_blocks,
    decay_total,
    state_low,
    conv_tail,
    taps,
    vectors,
    small,
    *rest,
):
    blocks = rest[:n_blocks]
    normed, raw_out, weighted_out, maps_out, logs_out = rest[n_blocks:]
    own, _, heads = decay_total.shape
    rows, width = weighted_out.shape
    props = rows // own
    bc = (conv_tail.shape[1] - width) // 2
    groups = bc // STATE
    group_width = width // groups
    total = None
    for block in blocks:
        for piece in [block[...]] if len(block.shape) == 2 else [block[i] for i in range(block.shape[0])]:
            piece = piece.astype(f32)
            total = piece if total is None else total + piece
    conv_width = width + 2 * bc
    tail = total[:, conv_width + width :]
    squares = tail[:, heads : heads + 1] + tail[:, heads + 1 : heads + 2]
    inv_rms = lax.rsqrt(squares / n_features + eps)
    raw = (total[:, :conv_width] * inv_rms).astype(bf16)
    raw_out[...] = raw
    raw = raw.astype(f32)
    gate = total[:, conv_width : conv_width + width] * inv_rms

    step_pre = tail[:, :heads] * inv_rms + small[0:1, :heads]
    step = jnp.maximum(step_pre, 0.0) + jnp.log1p(jnp.exp(-jnp.abs(step_pre)))
    totals = jnp.concatenate([decay_total[s] for s in range(own)], axis=0)
    logs = totals - small[1:2, :heads] * step
    logs_out[...] = logs
    step = spread(step, heads)
    decay = spread(jnp.exp(logs), heads)

    def turn(value, d):
        return pltpu.roll(value, d, 0)

    def since(size):
        return lax.rem(lax.broadcasted_iota(jnp.int32, (rows, size), 0), props)

    pos = since(conv_width)
    conv = conv_tail[...] + taps[CONV - 1 : CONV] * raw
    for d in range(1, CONV):
        conv = conv + jnp.where(pos >= d, taps[CONV - 1 - d : CONV - d] * turn(raw, d), 0.0)
    conv = silu(conv)
    x_conv = conv[:, :width]
    b_conv = conv[:, width : width + bc]
    c_conv = conv[:, width + bc :]
    maps_out[...] = b_conv
    weighted = step * x_conv
    weighted_out[...] = weighted

    pos = since(width)
    c_low = c_conv.astype(bf16)
    row_seq = lax.broadcasted_iota(jnp.int32, (rows, group_width), 0) // props
    from_state = []
    for g in range(groups):
        left = c_low[:, g * STATE : (g + 1) * STATE]
        out = None
        for s in range(own):
            part = lax.dot_general(
                left,
                state_low[s, g * group_width : (g + 1) * group_width, :],
                NT,
                preferred_element_type=f32,
            )
            out = part if out is None else jnp.where(row_seq >= s, part, out)
        from_state.append(out)
    from_state = jnp.concatenate(from_state, axis=1)

    span = decay
    to_start = decay
    heads_out = vectors[0:1] * x_conv
    for d in range(props):
        product = c_conv * (b_conv if d == 0 else turn(b_conv, d))
        scores = jnp.concatenate(
            [
                jnp.broadcast_to(
                    jnp.sum(product[:, g * STATE : (g + 1) * STATE], axis=1, keepdims=True),
                    (rows, group_width),
                )
                for g in range(groups)
            ],
            axis=1,
        )
        if d == 0:
            heads_out = heads_out + scores * weighted
        else:
            term = scores * span * turn(weighted, d)
            heads_out = heads_out + jnp.where(pos >= d, term, 0.0)
            span = span * turn(decay, d)
            to_start = jnp.where(pos >= d, span, to_start)
    heads_out = heads_out + to_start * from_state
    gated = heads_out * silu(gate)
    for g in range(groups):
        lanes = slice(g * group_width, (g + 1) * group_width)
        part = gated[:, lanes]
        mean = jnp.sum(part * part, axis=1, keepdims=True) / group_width
        normed[:, lanes] = (part * lax.rsqrt(mean + eps) * vectors[1:2, lanes]).astype(bf16)


def outputs_kernel(
    raw, weighted, maps, logs, tail_x, tail_maps, head_input, input_maps, log_decays, heads_window, maps_window
):
    own, props, width = head_input.shape
    bc = input_maps.shape[2]
    keep = CONV - 1
    heads_window[:keep] = tail_x[...]
    rows = raw[...].astype(f32)
    weighted, maps, logs = weighted[...], maps[...], logs[...]
    for s in range(own):
        mine = slice(s * props, (s + 1) * props)
        head_input[s] = weighted[mine].astype(bf16)
        input_maps[s] = maps[mine].astype(bf16)
        log_decays[s] = logs[mine]
        maps_window[s, :keep] = tail_maps[s]
        for t in range(props):
            r = s * props + t
            pair = [rows[r : r + 1, width : width + bc], rows[r : r + 1, width + bc :]]
            maps_window[s, keep + t] = jnp.concatenate(pair, axis=0).astype(bf16)
    for t in range(props):
        both = [rows[s * props + t : s * props + t + 1, :width] for s in range(own)]
        heads_window[keep + t] = jnp.concatenate(both, axis=0).astype(bf16)


def mix_kernel(n_kv, order, weight, *rest):
    blocks, out = rest[:-1], rest[-1]
    kv = lax.axis_index("kv")
    _, props, _ = out.shape
    pieces = []
    for block in blocks:
        pieces += [block[...]] if len(block.shape) == 2 else [block[i] for i in range(block.shape[0])]
    rows = pieces[0].shape[0]
    own = rows // props
    left = jnp.concatenate([piece.astype(f32) for piece in pieces], axis=0).astype(bf16)
    part = jnp.dot(left, weight[...], preferred_element_type=f32)
    for i, k in enumerate(order):
        start = peer(kv, k, n_kv, True, back=True) * own
        for s in range(own):
            at = i * rows + s * props
            out[start + s] = part[at : at + props].astype(bf16)


def local(
    tokens,
    input_norm_gain,
    head_input_weight,
    output_gate_weight,
    state_maps_weight,
    step_size_weight,
    step_size_bias,
    head_decay_speed,
    proposal_decay_total,
    head_input_kernel,
    state_maps_kernel,
    head_direct_gain,
    grouped_norm_gain,
    output_weight,
    prior_state_value,
    previous_head_input,
    previous_input_maps,
    previous_log_decays,
    prior_heads_window,
    prior_maps_window,
    accepted,
):
    n_kv, n_tp = lax.axis_size("kv"), lax.axis_size("tp")
    kv = lax.axis_index("kv")
    seqs, props, local_d = tokens.shape
    heads = step_size_weight.shape[1] // n_tp
    width = head_input_weight.shape[1]
    bc = state_maps_weight.shape[2]
    own = prior_state_value.shape[0]
    rows = own * props
    conv_width = width + 2 * bc
    packed = conv_width + width + LANES
    sds = jax.ShapeDtypeStruct
    vmem = pl.BlockSpec(memory_space=pltpu.VMEM)

    if local_d % LANES == 0:
        gain = input_norm_gain.reshape(-1, LANES)
        step_weight = step_size_weight.T
    else:
        gain = lax.dynamic_slice_in_dim(input_norm_gain, kv * local_d, local_d, 0)
        gain = gain.reshape(1, local_d)
        step_weight = lax.dynamic_slice_in_dim(step_size_weight.T, kv * local_d, local_d, 1)
    chunk = width
    n_copies = 3 + 2 * (width // chunk) + 1
    hbm = pl.BlockSpec(memory_space=pltpu.HBM)
    sent = pl.pallas_call(
        functools.partial(project_kernel, n_kv, n_tp, chunk),
        out_shape=[sds((rows, packed), bf16)] * n_kv,
        in_specs=[hbm] * 6,
        scratch_shapes=[
            pltpu.VMEM(tokens.shape, bf16),
            pltpu.VMEM(gain.shape, bf16),
            pltpu.VMEM(gain.shape, f32),
            pltpu.VMEM((step_weight.shape[0], local_d), bf16),
            pltpu.VMEM((n_kv * rows, LANES), f32),
            pltpu.VMEM((local_d, 2 * width), bf16),
            pltpu.VMEM((local_d, 2, bc), bf16),
            pltpu.SemaphoreType.DMA((n_copies,)),
        ],
        compiler_params=params(12),
        name="project",
    )(
        *(
            pltpu.with_memory_space_constraint(array, pltpu.HBM)
            for array in (
                tokens,
                gain,
                head_input_weight,
                state_maps_weight,
                output_gate_weight,
                step_weight,
            )
        )
    )
    if n_kv <= DIRECT:
        order = [*range(2, n_kv), *range(1, min(2, n_kv))]
        got = [permute(sent[k], "kv", k, n_kv) for k in order]
        got = [sent[0]] + got
    else:
        got = [lax.all_to_all(jnp.stack(sent), "kv", 0, 0)]

    later = (
        prior_state_value,
        previous_head_input,
        previous_input_maps,
        previous_log_decays,
        jnp.transpose(prior_heads_window, (1, 0, 2)),
        prior_maps_window,
        head_input_kernel,
        state_maps_kernel,
        step_size_bias.reshape(1, -1),
        head_decay_speed.reshape(1, -1),
        head_direct_gain.reshape(1, -1),
        grouped_norm_gain.reshape(-1, LANES),
    )
    (
        accepted_state,
        state_low,
        tail_x,
        tail_maps,
        conv_tail,
        taps,
        vectors,
        small,
    ) = pl.pallas_call(
        functools.partial(fetched_state_kernel, n_tp),
        out_shape=[
            sds(prior_state_value.shape, f32),
            sds((own, width, STATE), bf16),
            sds((CONV - 1, own, width), bf16),
            sds((own, CONV - 1, 2, bc), bf16),
            sds((rows, conv_width), f32),
            sds((CONV, conv_width), f32),
            sds((2, width), f32),
            sds((2, LANES), f32),
        ],
        in_specs=[pl.BlockSpec(memory_space=pltpu.SMEM)] + [hbm] * 12,
        scratch_shapes=[
            pltpu.VMEM((n_tp * width // LANES, LANES), f32),
            *(pltpu.VMEM(array.shape, array.dtype) for array in later),
            pltpu.SemaphoreType.DMA((len(later) - 1,)),
            pltpu.SemaphoreType.DMA((2, own)),
        ],
        out_specs=[hbm] + [vmem] * 7,
        compiler_params=params(12),
        name="state",
    )(accepted, *(pltpu.with_memory_space_constraint(array, pltpu.HBM) for array in later))

    normed, raw, weighted, maps, logs = pl.pallas_call(
        functools.partial(mixer_kernel, local_d * n_kv, len(got)),
        out_shape=[
            sds((rows, width), bf16),
            sds((rows, conv_width), bf16),
            sds((rows, width), f32),
            sds((rows, bc), f32),
            sds((rows, heads), f32),
        ],
        compiler_params=params(8),
        name="mixer",
    )(proposal_decay_total, state_low, conv_tail, taps, vectors, small, *got)

    if n_kv <= DIRECT:
        order = (0, *reversed(range(1, n_kv)))
        gathered = [normed] + [permute(normed, "kv", k, n_kv, True) for k in order[1:]]
    else:
        gathered = [lax.all_gather(normed, "kv")]
        order = tuple(range(n_kv))

    head_input, input_maps, log_decays, heads_window, maps_window = pl.pallas_call(
        outputs_kernel,
        out_shape=[
            sds((own, props, width), bf16),
            sds((own, props, bc), bf16),
            sds((own, props, heads), f32),
            sds((CONV - 1 + props, own, width), bf16),
            sds((own, CONV - 1 + props, 2, bc), bf16),
        ],
        compiler_params=params(8),
        name="outputs",
    )(raw, weighted, maps, logs, tail_x, tail_maps)

    part = pl.pallas_call(
        functools.partial(mix_kernel, n_kv, order),
        out_shape=sds((seqs, props, local_d), bf16),
        compiler_params=params(8),
        name="mix",
    )(output_weight, *gathered)
    total = part.astype(f32)
    for k in range(1, n_tp):
        total = total + permute(part, "tp", k, n_tp).astype(f32)
    return (
        total.astype(bf16),
        accepted_state,
        head_input,
        input_maps,
        log_decays,
        jnp.transpose(heads_window, (1, 0, 2)),
        maps_window,
    )


def solution(mesh):
    return jax.shard_map(
        local,
        mesh=mesh,
        in_specs=(
            P("dp", None, "kv"),
            P(),
            P("kv", "tp"),
            P("kv", "tp"),
            P("kv", None, "tp"),
            P(),
            P(),
            P(),
            P(("dp", "kv"), None, "tp"),
            P(),
            P(),
            P(),
            P(),
            P("tp", "kv"),
            P(("dp", "kv"), "tp", None, None),
            P(("dp", "kv"), None, "tp"),
            P(("dp", "kv"), None, "tp"),
            P(("dp", "kv"), None, "tp"),
            P(("dp", "kv"), None, "tp"),
            P(("dp", "kv"), None, None, "tp"),
            P(("dp", "kv")),
        ),
        out_specs=(
            P("dp", None, "kv"),
            P(("dp", "kv"), "tp", None, None),
            P(("dp", "kv"), None, "tp"),
            P(("dp", "kv"), None, "tp"),
            P(("dp", "kv"), None, "tp"),
            P(("dp", "kv"), None, "tp"),
            P(("dp", "kv"), None, None, "tp"),
        ),
        check_vma=False,
    )
```

```python
import functools

import jax
import jax.numpy as jnp
from jax import lax
from jax.experimental import pallas as pl
from jax.experimental.pallas import tpu as pltpu
from jax.sharding import PartitionSpec as P

HEAD_DIM = 64
STATE = 128
CONV = 4
LANES = 128
DIRECT = 8

eps = 1e-06
f32 = jnp.float32
bf16 = jnp.bfloat16

NT = (((1,), (1,)), ((), ()))
TN = (((0,), (0,)), ((), ()))


def params(mib):
    return pltpu.CompilerParams(vmem_limit_bytes=mib << 20)


def peer(me, k, n, ring, back=False):
    if n > DIRECT:
        return k
    if ring or n & (n - 1):
        at = me + (n - k if back else k)
        return at % n if isinstance(me, int) else lax.rem(at, n)
    return me ^ k


def permute(array, axis, k, n, ring=False):
    return lax.ppermute(array, axis, [(i, peer(i, k, n, ring)) for i in range(n)])


def pick(rows, index, count, width):
    out = rows[:, :width]
    for block in range(1, count):
        out = jnp.where(index == block, rows[:, block * width : (block + 1) * width], out)
    return out


def spread(values, heads):
    rows = values.shape[0]
    per = LANES // HEAD_DIM
    lane = lax.broadcasted_iota(jnp.int32, (rows, LANES), 1)
    tiles = []
    for first in range(0, heads, per):
        tile = jnp.broadcast_to(values[:, first : first + 1], (rows, LANES))
        for j in range(1, per):
            other = jnp.broadcast_to(values[:, first + j : first + j + 1], (rows, LANES))
            tile = jnp.where(lane >= j * HEAD_DIM, other, tile)
        tiles.append(tile)
    return jnp.concatenate(tiles, axis=1)


def silu(x):
    return x * (1.0 / (1.0 + jnp.exp(-x)))


def project_kernel(n_kv, n_tp, chunk, tok_hbm, gain_hbm, wx, wm, wg, ws_hbm, *rest):
    outs = rest[:n_kv]
    tok, gain, gain_rows, ws, step_rows, wide, pairs, sems = rest[n_kv:]
    kv, tp = lax.axis_index("kv"), lax.axis_index("tp")
    seqs, props, local_d = tok.shape
    own = seqs // n_kv
    rows = own * props
    width, bc = wx.shape[1], wm.shape[2]
    heads = ws.shape[0] // n_tp
    aligned = local_d % LANES == 0

    copies = []

    def fetch(source, target):
        copy = pltpu.make_async_copy(source, target, sems.at[len(copies)])
        copy.start()
        copies.append(copy)
        return copy

    small = [fetch(tok_hbm, tok), fetch(gain_hbm, gain)]
    columns = pl.ds(pl.multiple_of(kv * local_d, LANES), local_d) if aligned else slice(None)
    small.append(fetch(ws_hbm.at[:, columns], ws))
    maps = fetch(wm, pairs)
    plan = []
    for at in range(0, width, chunk):
        here = slice(at, at + chunk)
        plan.append((fetch(wx.at[:, here], wide.at[:, here]), at, here))
    for at in range(0, width, chunk):
        here = slice(width + at, width + at + chunk)
        plan.append((fetch(wg.at[:, at : at + chunk], wide.at[:, here]), width + 2 * bc + at, here))

    for copy in small:
        copy.wait()
    parts = []
    for k in range(n_kv):
        start = peer(kv, k, n_kv, False) * own
        for s in range(own):
            parts.append(tok[start + s].astype(f32))
    values = jnp.concatenate(parts, axis=0)
    squares = jnp.sum(values * values, axis=1, keepdims=True)
    gain_rows[...] = gain[...].astype(f32)
    if aligned:
        per = local_d // LANES
        factor = [gain_rows[pl.ds(kv * per + j, 1), :] for j in range(per)]
        factor = jnp.concatenate(factor, axis=1)
    else:
        factor = gain_rows[...]
    scaled = values * factor
    row = lax.broadcasted_iota(jnp.int32, (LANES, 2 * LANES), 0)
    column = lax.broadcasted_iota(jnp.int32, (LANES, 2 * LANES), 1)
    low = scaled.astype(bf16)
    apart = []
    for index in range(2):
        place = (column == 2 * row + index).astype(f32).astype(bf16)
        apart.append(
            jnp.concatenate(
                [
                    jnp.dot(low[:, at : at + LANES], place[: min(LANES, local_d), : 2 * min(LANES, local_d)], preferred_element_type=f32)
                    for at in range(0, local_d, LANES)
                ],
                axis=1,
            )
        )
    apart = jnp.concatenate(apart, axis=0).astype(bf16)

    high = squares.astype(bf16).astype(f32)
    step = lax.dot_general(low, ws[...], NT, preferred_element_type=f32)
    step_rows[...] = jnp.zeros_like(step_rows)
    step_rows[:, :heads] = pick(step, tp, n_tp, heads)
    step = step_rows[...]
    lane = lax.broadcasted_iota(jnp.int32, step.shape, 1)
    step = jnp.where(lane == heads, high, jnp.where(lane == heads + 1, squares - high, step))

    def put(at, part):
        for k in range(n_kv):
            piece = part[k * rows : (k + 1) * rows].astype(bf16)
            outs[k][:, at : at + part.shape[1]] = piece

    put(2 * width + 2 * bc, step)
    maps.wait()
    group = 2 * LANES if bc % (2 * LANES) == 0 else LANES
    for at in range(0, bc, group):
        block = [
            pairs[:, :, lane : lane + LANES].reshape(2 * local_d, LANES)
            for lane in range(at, at + group, LANES)
        ]
        both = jnp.dot(apart, jnp.concatenate(block, axis=1), preferred_element_type=f32)
        put(width + at, both[: n_kv * rows])
        put(width + bc + at, both[n_kv * rows :])
    count = len(plan) // 2
    for copy, at, here in plan[:count]:
        copy.wait()
        put(at, jnp.dot(low, wide[:, here], preferred_element_type=f32))
    for copy, at, here in plan[count:]:
        copy.wait()
        put(at, jnp.dot(low, wide[:, here], preferred_element_type=f32))


def state_kernel(
    n_tp,
    arrive,
    leave,
    acc,
    state,
    past_x,
    past_maps,
    past_logs,
    heads_window,
    maps_window,
    head_taps,
    map_taps,
    bias,
    speed,
    direct,
    norm_gain,
    state_low,
    tail_x,
    tail_maps,
    conv_tail,
    taps,
    vectors,
    small,
    gain_rows,
):
    tp = lax.axis_index("tp")
    own, heads = state.shape[:2]
    props, width = past_x.shape[1:]
    bc = past_maps.shape[2]
    groups = bc // STATE
    per_group = heads // groups
    group_width = per_group * HEAD_DIM
    keep = CONV - 1

    head_cols = pl.ds(pl.multiple_of(tp * width, LANES), width)
    map_cols = pl.ds(pl.multiple_of(tp * bc, LANES), bc)
    weight_x = head_taps[:, head_cols].astype(f32)
    taps[:, :width] = weight_x
    weight_b, weight_c = [], []
    for k in range(CONV):
        pair = map_taps[k, :, map_cols].astype(f32)
        weight_b.append(pair[0:1])
        weight_c.append(pair[1:2])
        taps[k : k + 1, width : width + bc] = pair[0:1]
        taps[k : k + 1, width + bc :] = pair[1:2]
    direct_half = pick(direct[...], tp, n_tp, heads)
    vectors[0:1, :] = spread(direct_half, heads)
    gain_rows[...] = norm_gain[...].astype(f32)
    per_row = width // LANES
    for j in range(per_row):
        vectors[1:2, j * LANES : (j + 1) * LANES] = gain_rows[pl.ds(tp * per_row + j, 1), :]
    small[0:1, :heads] = pick(bias[...], tp, n_tp, heads)
    small[1:2, :heads] = pick(speed[...], tp, n_tp, heads)

    for s in range(own):
        a = acc[s]
        xs, bs, cs = [], [], []
        for k in range(keep):
            row = heads_window[a + k].astype(f32)
            xs.append(row[s : s + 1])
            pair = maps_window[s, a + k]
            tail_maps[s, k] = pair
            pair = pair.astype(f32)
            bs.append(pair[0:1])
            cs.append(pair[1:2])
        for k in range(keep):
            tail_x[k, s : s + 1, :] = xs[k].astype(bf16)
        for at, weights, rows in (
            (0, [weight_x[k : k + 1] for k in range(CONV)], xs),
            (width, weight_b, bs),
            (width + bc, weight_c, cs),
        ):
            size = rows[0].shape[1]
            for t in range(props):
                total = jnp.zeros((1, size), f32)
                for k in range(CONV):
                    if t + k < keep:
                        total = total + weights[k] * rows[t + k]
                conv_tail[s * props + t : s * props + t + 1, at : at + size] = total

        logs = past_logs[s]
        after = jnp.zeros((1, heads), f32)
        coefficients = [None] * props
        for j in reversed(range(props)):
            coefficients[j] = jnp.where(j < a, jnp.exp(after), 0.0)
            after = after + jnp.where(j < a, logs[j : j + 1], 0.0)
        factor = jnp.exp(after)
        arrive(s)
        coefficient = spread(jnp.concatenate(coefficients, axis=0), heads)
        scaled = past_x[s].astype(f32) * coefficient
        high = scaled.astype(bf16).astype(f32)
        left = jnp.concatenate([high, scaled - high], axis=0)
        maps = past_maps[s].astype(f32)
        maps = jnp.concatenate([maps, maps], axis=0).astype(bf16)
        for g in range(groups):
            block = left[:, g * group_width : (g + 1) * group_width]
            update = lax.dot_general(
                block.astype(bf16),
                maps[:, g * STATE : (g + 1) * STATE],
                TN,
                preferred_element_type=f32,
            )
            for i in range(per_group):
                h = g * per_group + i
                value = state[s, h] * factor[:, h : h + 1]
                value = value + update[i * HEAD_DIM : (i + 1) * HEAD_DIM]
                state[s, h] = value
                state_low[s, h * HEAD_DIM : (h + 1) * HEAD_DIM, :] = value.astype(bf16)
            leave(s, g * per_group, per_group)


def fetched_state_kernel(n_tp, acc, state_hbm, *rest):
    sources, new_state, outs, rest = rest[:11], rest[11], rest[12:19], rest[19:]
    gain_rows, state, targets = rest[0], rest[1], rest[2:13]
    sems, state_sems, out_sems = rest[13:]
    own = state.shape[0]
    small = [
        pltpu.make_async_copy(source, target, sems.at[i])
        for i, (source, target) in enumerate(zip(sources, targets, strict=True))
    ]
    inward = [
        pltpu.make_async_copy(state_hbm.at[s], state.at[s], state_sems.at[s])
        for s in range(own)
    ]
    outward = []

    def leave(s, first, count):
        part = pl.ds(first, count)
        copy = pltpu.make_async_copy(
            state.at[s, part], new_state.at[s, part], out_sems.at[len(outward)]
        )
        copy.start()
        outward.append(copy)

    for copy in small + inward:
        copy.start()
    for copy in small:
        copy.wait()
    state_kernel(
        n_tp,
        lambda s: inward[s].wait(),
        leave,
        acc,
        state,
        *targets,
        *outs,
        gain_rows,
    )
    for copy in outward:
        copy.wait()


def mixer_kernel(
    n_features,
    n_blocks,
    decay_total,
    state_low,
    conv_tail,
    taps,
    vectors,
    small,
    *rest,
):
    blocks = rest[:n_blocks]
    normed, raw_out, weighted_out, maps_out, logs_out = rest[n_blocks:]
    own, _, heads = decay_total.shape
    rows, width = weighted_out.shape
    props = rows // own
    bc = (conv_tail.shape[1] - width) // 2
    groups = bc // STATE
    group_width = width // groups
    total = None
    for block in blocks:
        for piece in [block[...]] if len(block.shape) == 2 else [block[i] for i in range(block.shape[0])]:
            piece = piece.astype(f32)
            total = piece if total is None else total + piece
    conv_width = width + 2 * bc
    tail = total[:, conv_width + width :]
    squares = tail[:, heads : heads + 1] + tail[:, heads + 1 : heads + 2]
    inv_rms = lax.rsqrt(squares / n_features + eps)
    raw = (total[:, :conv_width] * inv_rms).astype(bf16)
    raw_out[...] = raw
    raw = raw.astype(f32)
    gate = total[:, conv_width : conv_width + width] * inv_rms

    step_pre = tail[:, :heads] * inv_rms + small[0:1, :heads]
    step = jnp.maximum(step_pre, 0.0) + jnp.log1p(jnp.exp(-jnp.abs(step_pre)))
    totals = jnp.concatenate([decay_total[s] for s in range(own)], axis=0)
    logs = totals - small[1:2, :heads] * step
    logs_out[...] = logs
    step = spread(step, heads)
    decay = spread(jnp.exp(logs), heads)

    def turn(value, d):
        return pltpu.roll(value, d, 0)

    def since(size):
        return lax.rem(lax.broadcasted_iota(jnp.int32, (rows, size), 0), props)

    pos = since(conv_width)
    conv = conv_tail[...] + taps[CONV - 1 : CONV] * raw
    for d in range(1, CONV):
        conv = conv + jnp.where(pos >= d, taps[CONV - 1 - d : CONV - d] * turn(raw, d), 0.0)
    conv = silu(conv)
    x_conv = conv[:, :width]
    b_conv = conv[:, width : width + bc]
    c_conv = conv[:, width + bc :]
    maps_out[...] = b_conv
    weighted = step * x_conv
    weighted_out[...] = weighted

    pos = since(width)
    c_low = c_conv.astype(bf16)
    row_seq = lax.broadcasted_iota(jnp.int32, (rows, group_width), 0) // props
    from_state = []
    for g in range(groups):
        left = c_low[:, g * STATE : (g + 1) * STATE]
        out = None
        for s in range(own):
            part = lax.dot_general(
                left,
                state_low[s, g * group_width : (g + 1) * group_width, :],
                NT,
                preferred_element_type=f32,
            )
            out = part if out is None else jnp.where(row_seq >= s, part, out)
        from_state.append(out)
    from_state = jnp.concatenate(from_state, axis=1)

    span = decay
    to_start = decay
    heads_out = vectors[0:1] * x_conv
    for d in range(props):
        product = c_conv * (b_conv if d == 0 else turn(b_conv, d))
        scores = jnp.concatenate(
            [
                jnp.broadcast_to(
                    jnp.sum(product[:, g * STATE : (g + 1) * STATE], axis=1, keepdims=True),
                    (rows, group_width),
                )
                for g in range(groups)
            ],
            axis=1,
        )
        if d == 0:
            heads_out = heads_out + scores * weighted
        else:
            term = scores * span * turn(weighted, d)
            heads_out = heads_out + jnp.where(pos >= d, term, 0.0)
            span = span * turn(decay, d)
            to_start = jnp.where(pos >= d, span, to_start)
    heads_out = heads_out + to_start * from_state
    gated = heads_out * silu(gate)
    for g in range(groups):
        lanes = slice(g * group_width, (g + 1) * group_width)
        part = gated[:, lanes]
        mean = jnp.sum(part * part, axis=1, keepdims=True) / group_width
        normed[:, lanes] = (part * lax.rsqrt(mean + eps) * vectors[1:2, lanes]).astype(bf16)


def outputs_kernel(
    raw, weighted, maps, logs, tail_x, tail_maps, head_input, input_maps, log_decays, heads_window, maps_window
):
    own, props, width = head_input.shape
    bc = input_maps.shape[2]
    keep = CONV - 1
    heads_window[:keep] = tail_x[...]
    rows = raw[...].astype(f32)
    weighted, maps, logs = weighted[...], maps[...], logs[...]
    for s in range(own):
        mine = slice(s * props, (s + 1) * props)
        head_input[s] = weighted[mine].astype(bf16)
        input_maps[s] = maps[mine].astype(bf16)
        log_decays[s] = logs[mine]
        maps_window[s, :keep] = tail_maps[s]
        for t in range(props):
            r = s * props + t
            pair = [rows[r : r + 1, width : width + bc], rows[r : r + 1, width + bc :]]
            maps_window[s, keep + t] = jnp.concatenate(pair, axis=0).astype(bf16)
    for t in range(props):
        both = [rows[s * props + t : s * props + t + 1, :width] for s in range(own)]
        heads_window[keep + t] = jnp.concatenate(both, axis=0).astype(bf16)


def mix_kernel(n_kv, order, weight, *rest):
    blocks, out = rest[:-1], rest[-1]
    kv = lax.axis_index("kv")
    _, props, _ = out.shape
    pieces = []
    for block in blocks:
        pieces += [block[...]] if len(block.shape) == 2 else [block[i] for i in range(block.shape[0])]
    rows = pieces[0].shape[0]
    own = rows // props
    left = jnp.concatenate([piece.astype(f32) for piece in pieces], axis=0).astype(bf16)
    part = jnp.dot(left, weight[...], preferred_element_type=f32)
    for i, k in enumerate(order):
        start = peer(kv, k, n_kv, True, back=True) * own
        for s in range(own):
            at = i * rows + s * props
            out[start + s] = part[at : at + props].astype(bf16)


def local(
    tokens,
    input_norm_gain,
    head_input_weight,
    output_gate_weight,
    state_maps_weight,
    step_size_weight,
    step_size_bias,
    head_decay_speed,
    proposal_decay_total,
    head_input_kernel,
    state_maps_kernel,
    head_direct_gain,
    grouped_norm_gain,
    output_weight,
    prior_state_value,
    previous_head_input,
    previous_input_maps,
    previous_log_decays,
    prior_heads_window,
    prior_maps_window,
    accepted,
):
    n_kv, n_tp = lax.axis_size("kv"), lax.axis_size("tp")
    kv = lax.axis_index("kv")
    seqs, props, local_d = tokens.shape
    heads = step_size_weight.shape[1] // n_tp
    width = head_input_weight.shape[1]
    bc = state_maps_weight.shape[2]
    own = prior_state_value.shape[0]
    rows = own * props
    conv_width = width + 2 * bc
    packed = conv_width + width + LANES
    sds = jax.ShapeDtypeStruct
    vmem = pl.BlockSpec(memory_space=pltpu.VMEM)

    if local_d % LANES == 0:
        gain = input_norm_gain.reshape(-1, LANES)
        step_weight = step_size_weight.T
    else:
        gain = lax.dynamic_slice_in_dim(input_norm_gain, kv * local_d, local_d, 0)
        gain = gain.reshape(1, local_d)
        step_weight = lax.dynamic_slice_in_dim(step_size_weight.T, kv * local_d, local_d, 1)
    chunk = width
    n_copies = 3 + 2 * (width // chunk) + 1
    hbm = pl.BlockSpec(memory_space=pltpu.HBM)
    sent = pl.pallas_call(
        functools.partial(project_kernel, n_kv, n_tp, chunk),
        out_shape=[sds((rows, packed), bf16)] * n_kv,
        in_specs=[hbm] * 6,
        scratch_shapes=[
            pltpu.VMEM(tokens.shape, bf16),
            pltpu.VMEM(gain.shape, bf16),
            pltpu.VMEM(gain.shape, f32),
            pltpu.VMEM((step_weight.shape[0], local_d), bf16),
            pltpu.VMEM((n_kv * rows, LANES), f32),
            pltpu.VMEM((local_d, 2 * width), bf16),
            pltpu.VMEM((local_d, 2, bc), bf16),
            pltpu.SemaphoreType.DMA((n_copies,)),
        ],
        compiler_params=params(12),
        name="project",
    )(
        *(
            pltpu.with_memory_space_constraint(array, pltpu.HBM)
            for array in (
                tokens,
                gain,
                head_input_weight,
                state_maps_weight,
                output_gate_weight,
                step_weight,
            )
        )
    )
    if n_kv <= DIRECT:
        order = [*range(2, n_kv), *range(1, min(2, n_kv))]
        got = [permute(sent[k], "kv", k, n_kv) for k in order]
        got = [sent[0]] + got
    else:
        got = [lax.all_to_all(jnp.stack(sent), "kv", 0, 0)]

    later = (
        prior_state_value,
        previous_head_input,
        previous_input_maps,
        previous_log_decays,
        jnp.transpose(prior_heads_window, (1, 0, 2)),
        prior_maps_window,
        head_input_kernel,
        state_maps_kernel,
        step_size_bias.reshape(1, -1),
        head_decay_speed.reshape(1, -1),
        head_direct_gain.reshape(1, -1),
        grouped_norm_gain.reshape(-1, LANES),
    )
    (
        accepted_state,
        state_low,
        tail_x,
        tail_maps,
        conv_tail,
        taps,
        vectors,
        small,
    ) = pl.pallas_call(
        functools.partial(fetched_state_kernel, n_tp),
        out_shape=[
            sds(prior_state_value.shape, f32),
            sds((own, width, STATE), bf16),
            sds((CONV - 1, own, width), bf16),
            sds((own, CONV - 1, 2, bc), bf16),
            sds((rows, conv_width), f32),
            sds((CONV, conv_width), f32),
            sds((2, width), f32),
            sds((2, LANES), f32),
        ],
        in_specs=[pl.BlockSpec(memory_space=pltpu.SMEM)] + [hbm] * 12,
        scratch_shapes=[
            pltpu.VMEM((n_tp * width // LANES, LANES), f32),
            *(pltpu.VMEM(array.shape, array.dtype) for array in later),
            pltpu.SemaphoreType.DMA((len(later) - 1,)),
            pltpu.SemaphoreType.DMA((own,)),
            pltpu.SemaphoreType.DMA((own * (bc // STATE),)),
        ],
        out_specs=[hbm] + [vmem] * 7,
        compiler_params=params(12),
        name="state",
    )(accepted, *(pltpu.with_memory_space_constraint(array, pltpu.HBM) for array in later))

    normed, raw, weighted, maps, logs = pl.pallas_call(
        functools.partial(mixer_kernel, local_d * n_kv, len(got)),
        out_shape=[
            sds((rows, width), bf16),
            sds((rows, conv_width), bf16),
            sds((rows, width), f32),
            sds((rows, bc), f32),
            sds((rows, heads), f32),
        ],
        compiler_params=params(8),
        name="mixer",
    )(proposal_decay_total, state_low, conv_tail, taps, vectors, small, *got)

    if n_kv <= DIRECT:
        order = (0, *reversed(range(1, n_kv)))
        gathered = [normed] + [permute(normed, "kv", k, n_kv, True) for k in order[1:]]
    else:
        gathered = [lax.all_gather(normed, "kv")]
        order = tuple(range(n_kv))

    head_input, input_maps, log_decays, heads_window, maps_window = pl.pallas_call(
        outputs_kernel,
        out_shape=[
            sds((own, props, width), bf16),
            sds((own, props, bc), bf16),
            sds((own, props, heads), f32),
            sds((CONV - 1 + props, own, width), bf16),
            sds((own, CONV - 1 + props, 2, bc), bf16),
        ],
        compiler_params=params(8),
        name="outputs",
    )(raw, weighted, maps, logs, tail_x, tail_maps)

    part = pl.pallas_call(
        functools.partial(mix_kernel, n_kv, order),
        out_shape=sds((seqs, props, local_d), bf16),
        compiler_params=params(8),
        name="mix",
    )(output_weight, *gathered)
    total = part.astype(f32)
    for k in range(1, n_tp):
        total = total + permute(part, "tp", k, n_tp).astype(f32)
    return (
        total.astype(bf16),
        accepted_state,
        head_input,
        input_maps,
        log_decays,
        jnp.transpose(heads_window, (1, 0, 2)),
        maps_window,
    )


def solution(mesh):
    return jax.shard_map(
        local,
        mesh=mesh,
        in_specs=(
            P("dp", None, "kv"),
            P(),
            P("kv", "tp"),
            P("kv", "tp"),
            P("kv", None, "tp"),
            P(),
            P(),
            P(),
            P(("dp", "kv"), None, "tp"),
            P(),
            P(),
            P(),
            P(),
            P("tp", "kv"),
            P(("dp", "kv"), "tp", None, None),
            P(("dp", "kv"), None, "tp"),
            P(("dp", "kv"), None, "tp"),
            P(("dp", "kv"), None, "tp"),
            P(("dp", "kv"), None, "tp"),
            P(("dp", "kv"), None, None, "tp"),
            P(("dp", "kv")),
        ),
        out_specs=(
            P("dp", None, "kv"),
            P(("dp", "kv"), "tp", None, None),
            P(("dp", "kv"), None, "tp"),
            P(("dp", "kv"), None, "tp"),
            P(("dp", "kv"), None, "tp"),
            P(("dp", "kv"), None, "tp"),
            P(("dp", "kv"), None, None, "tp"),
        ),
        check_vma=False,
    )
```
